32 devices in a mesh: sp: 16 (over z, y, x), tp: 2 (over core).
Axes of the slice: x: 2, y: 2, z: 4, core: 2. Of those that a mesh axis runs over, the one named last changes fastest.
Arguments:
- queries: bfloat16 [4096, 512], P('sp', 'tp'), may hold values from -20 to 20
- key_rows: bfloat16 [4096, 512], P('sp', 'tp'), may hold values from -20 to 20
- value_rows: bfloat16 [4096, 512], P('sp', 'tp'), may hold values from -6 to 6
- residual: bfloat16 [4096, 2048], P(('sp', 'tp')), may hold values from -6 to 6
- out_weight: bfloat16 [512, 2048], replicated, may hold values from -0.75 to 0.75
- norm_gain: float32 [2048], replicated, may hold values from 0.1 to 1.9
- routes: int32 [4096, 8], P(('sp', 'tp')), may hold values from 0 to 15, all different within a row; in each aligned block of 128 rows (0 to 127, 128 to 255, ...) at most 80 rows name the same one
- route_weight: float32 [4096, 8], P(('sp', 'tp')), may hold values from 0.1 to 0.6
- expert_gate: bfloat16 [16, 2048, 512], P('sp', None, 'tp'), may hold values from -0.125 to 0.125
- expert_up: bfloat16 [16, 2048, 512], P('sp', None, 'tp'), may hold values from -0.125 to 0.125
- expert_down: bfloat16 [16, 512, 2048], P('sp', 'tp'), may hold values from -0.25 to 0.25
- shared_gate: bfloat16 [2048, 512], replicated, may hold values from -0.125 to 0.125
- shared_up: bfloat16 [2048, 512], replicated, may hold values from -0.125 to 0.125
- shared_down: bfloat16 [512, 2048], replicated, may hold values from -0.25 to 0.25
Outputs:
- output: bfloat16 [4096, 2048], P(('sp', 'tp'))
The draws below stay inside these ranges and needn't reach their ends.
Inputs may be any that keep to these rules, and one draw needn't show every extreme that they name: `routes`: each row names 8 different experts. In each aligned block of 128 rows (the rows of one device) no expert is named more than 80 times, a bound that some block reaches.
All inputs are finite; a program needn't handle non-finite values.
Results may differ from the reference program's by a relative error of at most 0.012.
Values may be sent and summed in bfloat16 or wider, within the bound.
A program may use at most 192 MiB of HBM per device.

```python
import math
import jax
import jax.numpy as jnp
import numpy as np
from jax import lax

D = 2048
FOCUS_CHANNELS = 8
HEAD_DIM = 64
FFE = 512
SHARED = 512
TOPK = 8
TOK_DEV = 256
STRING_ITEMS = 4096
ATT = 512
EXPERTS = 16
CAP = 80
N_TP = 2


def channel_arrangement(key):
    starting_shift = jax.random.fold_in(key, 101)
    heading_seed, layering_seed, permuting_seed, segment_seed, cluster_seed = jax.random.split(starting_shift, 5)
    movement_heading = jax.random.normal(heading_seed, (FOCUS_CHANNELS, HEAD_DIM), jnp.float32)
    movement_heading = movement_heading / jnp.sqrt(jnp.sum(movement_heading * movement_heading, axis=1, keepdims=True))
    order = jax.random.permutation(permuting_seed, FOCUS_CHANNELS)
    quick = order < FOCUS_CHANNELS // 2
    slow_depth = jax.random.uniform(layering_seed, (FOCUS_CHANNELS,), jnp.float32, 11.5, 13.0)
    quick_depth = jax.random.uniform(jax.random.fold_in(layering_seed, 1), (FOCUS_CHANNELS,), jnp.float32, 3.5, 5.0)
    layering_count = jnp.where(quick, quick_depth, slow_depth)
    segment_multiplier = jax.random.uniform(segment_seed, (STRING_ITEMS // TOK_DEV, FOCUS_CHANNELS), jnp.float32, 0.92, 1.08)
    cluster_count = jax.random.randint(cluster_seed, (4, FOCUS_CHANNELS), 0, STRING_ITEMS)
    return (movement_heading, layering_count, segment_multiplier, cluster_count)


def draw_queries(key, part):
    movement_heading, layering_count, segment_multiplier, cluster_count = channel_arrangement(key)
    noise_key = jax.random.fold_in(key, 202)
    noise = 0.5 * jnp.clip(jax.random.normal(noise_key, (STRING_ITEMS, FOCUS_CHANNELS, HEAD_DIM), jnp.float32), -5.0, 5.0)
    rows = layering_count[None, :, None] * movement_heading[None, :, :] + noise
    return rows.reshape(STRING_ITEMS, FOCUS_CHANNELS * HEAD_DIM).astype(jnp.bfloat16)


def draw_key_rows(key, part):
    movement_heading, layering_count, segment_multiplier, cluster_count = channel_arrangement(key)
    noise_key = jax.random.fold_in(key, 303)
    item_indices = jnp.arange(STRING_ITEMS, dtype=jnp.int32)
    strength = 8.0 * segment_multiplier[item_indices // TOK_DEV]
    broken_entries = jnp.any(item_indices[:, None, None] == cluster_count[None, :, :], axis=1)
    strength = jnp.where(broken_entries, 5.6 / layering_count[None, :], strength)
    noise = jnp.clip(jax.random.normal(noise_key, (STRING_ITEMS, FOCUS_CHANNELS, HEAD_DIM), jnp.float32), -5.0, 5.0)
    rows = noise - strength[:, :, None] * movement_heading[None, :, :]
    return rows.reshape(STRING_ITEMS, FOCUS_CHANNELS * HEAD_DIM).astype(jnp.bfloat16)


def shard_levels(own_key, dims, cuts, low, high):
    loudness = 1.0
    for dim, blocks in cuts:
        steps = jax.random.uniform(jax.random.fold_in(jax.random.fold_in(own_key, 6), dim), (blocks,), jnp.float32, low / len(cuts), high / len(cuts))
        loudness = loudness * jnp.repeat(jnp.exp(steps), dims[dim] // blocks).reshape((-1,) + (1,) * (len(dims) - 1 - dim))
    return loudness


def routed_block(key, own, number, rows, number_of, top, bound, skew):
    order = jax.random.permutation(key, number_of)
    heavy_load, usual = load_shares(number_of, rows * top, bound, skew, True), load_shares(number_of, rows * top, bound, skew, False)
    places = jnp.arange(number_of)

    def named(lengths, rotation):
        used = int((lengths > 0).sum())
        fixed = max(1, used // 4)
        shifted = fixed + (places - fixed + rotation * (used - fixed)) % max(1, number_of - fixed)
        return jnp.zeros((number_of,), jnp.int32).at[order[jnp.where(places < fixed, places, shifted)]].set(jnp.asarray(lengths, jnp.int32))

    lengths = jnp.where(number % 4 == 0, named(heavy_load, number // 4), named(usual, number - number // 4 - 1))
    mixed = jax.random.permutation(jax.random.fold_in(own, 3), number_of)
    source_of, receiver = mixed[0:number_of // 2 * 2:2], mixed[1:number_of // 2 * 2:2]
    room = jnp.minimum(lengths[source_of] - 1, bound - lengths[receiver]) // 2
    room = jnp.where((source_of == order[0]) | (receiver == order[0]) | (lengths[receiver] == 0), 0, jnp.maximum(room, 0))
    shifted = jax.random.randint(jax.random.fold_in(own, 4), (number_of // 2,), 0, 1 << 20) % (room + 1)
    lengths = lengths.at[source_of].add(-shifted).at[receiver].add(shifted)
    items = jnp.searchsorted(jnp.cumsum(lengths), jnp.arange(rows * top), side="right").astype(jnp.int32)
    grid = items.reshape(top, rows).T
    grid = grid[jax.random.permutation(jax.random.fold_in(own, 1), rows)]
    rotation = jax.random.randint(jax.random.fold_in(own, 2), (rows, 1), 0, top)
    return jnp.take_along_axis(grid, (jnp.arange(top)[None, :] + rotation) % top, axis=1)


def load_shares(count, total, reach, lean, full):
    loads = [(1 << 20) // math.isqrt(rank ** lean) + 1 for rank in range(1, count + 1)]
    largest = reach if full else min(reach, max(-(-total // count), total * loads[0] // sum(loads)))
    least = 1 if total - largest >= count - 1 else 0
    counts, spare = [largest] + [least] * (count - 1), total - largest - least * (count - 1)
    while spare > 0:
        candidates = [i for i in range(1, count) if counts[i] < largest] or [i for i in range(1, count) if counts[i] < reach]
        whole, budget = sum([loads[i] for i in candidates]), spare
        for i in candidates:
            addition = min(reach - counts[i], max(1, budget * loads[i] // whole), spare)
            counts[i] = counts[i] + addition
            spare = spare - addition
    return np.array(counts)


def scatter_about(stream_key, shape, deviation, most, shards=(), held_as=jnp.bfloat16):
    values = jax.random.normal(stream_key, shape, jnp.float32) * deviation
    if len(shards) > 0:
        values = shard_levels(stream_key, shape, shards, -0.22, 0.18) * values
    return jnp.clip(values, min=-most, max=most).astype(held_as)


def setup_inputs(seed: int = 0) -> dict:
    seeds = jax.random.split(jax.random.key(seed), 15)
    queries = draw_queries(jax.random.fold_in(seeds[14], 71), 0)
    key_rows = draw_key_rows(jax.random.fold_in(seeds[14], 71), 0)
    value_rows = scatter_about(seeds[2], (STRING_ITEMS, ATT), 1.0, 6.0, ((0, 16), (1, 2)))
    residual = scatter_about(seeds[3], (STRING_ITEMS, D), 1.0, 6.0, ((0, 32),))
    out_weight = scatter_about(seeds[4], (ATT, D), (ATT // 9) ** -0.5, 0.75)
    norm_gain = jnp.clip(1.0 + 0.18 * jax.random.normal(seeds[5], (D,), jnp.float32), 0.1, 1.9)
    routes_keys = jax.random.split(jax.random.fold_in(seeds[6], 1), STRING_ITEMS // (TOK_DEV // N_TP))
    routes_turns = jax.random.permutation(jax.random.fold_in(seeds[6], 3), STRING_ITEMS // (TOK_DEV // N_TP))
    routes = jax.vmap(lambda own, number: routed_block(jax.random.fold_in(seeds[6], 2), own, number, TOK_DEV // N_TP, EXPERTS, TOPK, CAP, 1))(routes_keys, routes_turns).reshape((STRING_ITEMS, TOPK))
    route_weight = jnp.clip(jnp.exp(math.log(0.6) - 1.7917595 * jax.random.uniform(seeds[7], (STRING_ITEMS, TOPK), jnp.float32) ** shard_levels(seeds[7], (STRING_ITEMS, TOPK), ((0, 32),), -0.2, 0.2)), 0.1, 0.6)
    expert_gate = scatter_about(seeds[8], (EXPERTS, D, FFE), D ** -0.5, 0.125, ((0, 16), (2, 2)))
    expert_up = scatter_about(seeds[9], (EXPERTS, D, FFE), D ** -0.5, 0.125, ((0, 16), (2, 2)))
    expert_down = scatter_about(seeds[10], (EXPERTS, FFE, D), FFE ** -0.5, 0.25, ((0, 16), (1, 2)))
    shared_gate = scatter_about(seeds[11], (D, SHARED), D ** -0.5, 0.125)
    shared_up = scatter_about(seeds[12], (D, SHARED), D ** -0.5, 0.125)
    shared_down = scatter_about(seeds[13], (SHARED, D), SHARED ** -0.5, 0.25)
    return {"queries": queries, "key_rows": key_rows, "value_rows": value_rows, "residual": residual, "out_weight": out_weight, "norm_gain": norm_gain, "routes": routes, "route_weight": route_weight, "expert_gate": expert_gate, "expert_up": expert_up, "expert_down": expert_down, "shared_gate": shared_gate, "shared_up": shared_up, "shared_down": shared_down}


def reference(queries, key_rows, value_rows, residual, out_weight, norm_gain, routes, route_weight, expert_gate, expert_up, expert_down, shared_gate, shared_up, shared_down):
    factor = HEAD_DIM ** (-0.5)
    blocks = STRING_ITEMS // TOK_DEV
    key_heads = key_rows.astype(jnp.float32).reshape(blocks, TOK_DEV, FOCUS_CHANNELS, HEAD_DIM)
    value_heads = value_rows.astype(jnp.float32).reshape(blocks, TOK_DEV, FOCUS_CHANNELS, HEAD_DIM)
    key_pos = jnp.arange(STRING_ITEMS, dtype=jnp.int32).reshape(blocks, TOK_DEV)

    def query_block(index):
        query_heads = lax.dynamic_slice_in_dim(queries, index * TOK_DEV, TOK_DEV, 0).astype(jnp.float32).reshape(TOK_DEV, FOCUS_CHANNELS, HEAD_DIM)
        scores = jnp.einsum('thd,bshd->hbts', query_heads, key_heads, precision=lax.Precision.HIGHEST) * factor
        query_pos = index * TOK_DEV + jnp.arange(TOK_DEV, dtype=jnp.int32)
        live = key_pos[None, :, None, :] < query_pos[None, None, :, None]
        cost = jnp.where(live, jax.nn.softplus(scores), 0.0)
        inside = lax.cumsum(cost, axis=3, reverse=True) - cost
        weight = jnp.where(live, jnp.exp(jax.nn.log_sigmoid(scores) - inside), 0.0).astype(jnp.bfloat16)
        partial_value = jnp.einsum('hbts,bshd->bthd', weight.astype(jnp.float32), value_heads, precision=lax.Precision.HIGHEST)
        total = lax.optimization_barrier(jnp.sum(cost, axis=3))
        later = lax.cumsum(total, axis=1, reverse=True) - total
        attended = jnp.einsum('hbt,bthd->thd', jnp.exp(-later), partial_value, precision=lax.Precision.HIGHEST)
        return attended.reshape(TOK_DEV, ATT).astype(jnp.bfloat16)
    attended = lax.map(query_block, jnp.arange(blocks, dtype=jnp.int32)).reshape(STRING_ITEMS, ATT)
    projected = jnp.dot(attended, out_weight, preferred_element_type=jnp.float32)
    mixed = (residual.astype(jnp.float32) + projected).astype(jnp.bfloat16)
    mixed_wide = mixed.astype(jnp.float32)
    inverse = lax.rsqrt(lax.optimization_barrier(jnp.mean(mixed_wide * mixed_wide, axis=1, keepdims=True)) + 1e-06)
    normed = (mixed_wide * inverse * norm_gain.astype(jnp.float32)).astype(jnp.bfloat16)
    row_count = TOK_DEV // N_TP
    sources = STRING_ITEMS // row_count

    def slots(block_routes):
        flat = block_routes.reshape(-1)
        picks = (flat[:, None] == jnp.arange(EXPERTS, dtype=jnp.int32)[None, :]).astype(jnp.int32)
        earlier = jnp.cumsum(picks, axis=0) - picks
        return flat * CAP + lax.optimization_barrier(jnp.sum(earlier * picks, axis=1))
    position = lax.map(slots, routes.reshape(sources, row_count, TOPK))
    flat_slot = (jnp.arange(sources, dtype=jnp.int32)[:, None] * (EXPERTS * CAP) + position).reshape(-1)
    filler = jnp.zeros((sources * EXPERTS * CAP,), jnp.int32).at[flat_slot].set(jnp.arange(STRING_ITEMS * TOPK, dtype=jnp.int32) + 1)
    filler = filler.reshape(sources, EXPERTS, CAP).transpose(1, 0, 2).reshape(EXPERTS, sources * CAP)
    flat_weight = route_weight.reshape(-1)
    half = FFE // N_TP

    def one_expert(accum, inputs):
        fill_row, gate_matrix, up_matrix, down_matrix = inputs
        occupied = fill_row > 0
        assignment = jnp.maximum(fill_row - 1, 0)
        token_index = assignment // TOPK
        rows_in = normed[token_index]
        summed = jnp.zeros((rows_in.shape[0], D), jnp.float32)
        for section in range(N_TP):
            gate = jnp.dot(rows_in, gate_matrix[:, section * half:(section + 1) * half], preferred_element_type=jnp.float32)
            upward = jnp.dot(rows_in, up_matrix[:, section * half:(section + 1) * half], preferred_element_type=jnp.float32)
            hidden = (jax.nn.silu(gate) * upward).astype(jnp.bfloat16)
            result = jnp.dot(hidden, down_matrix[section * half:(section + 1) * half], preferred_element_type=jnp.float32)
            summed = summed + lax.optimization_barrier(result.astype(jnp.bfloat16)).astype(jnp.float32)
        expert_out = lax.optimization_barrier(summed.astype(jnp.bfloat16)).astype(jnp.float32)
        contribution = jnp.where(occupied[:, None], expert_out * flat_weight[assignment][:, None], 0.0)
        return (accum.at[token_index].add(contribution), None)
    routed, _ = lax.scan(one_expert, jnp.zeros((STRING_ITEMS, D), jnp.float32), (filler, expert_gate, expert_up, expert_down))
    shared_gate_out = jnp.dot(normed, shared_gate, preferred_element_type=jnp.float32)
    shared_up_out = jnp.dot(normed, shared_up, preferred_element_type=jnp.float32)
    shared_act = (jax.nn.silu(shared_gate_out) * shared_up_out).astype(jnp.bfloat16)
    shared_out = jnp.dot(shared_act, shared_down, preferred_element_type=jnp.float32)
    return (mixed_wide + routed + shared_out).astype(jnp.bfloat16)
```

```python
import functools

import jax
import jax.numpy as jnp
from jax import lax
from jax.experimental import pallas as pl
from jax.experimental.pallas import tpu as pltpu
from jax.sharding import PartitionSpec as P

HEAD_DIM = 64
TOPK = 8


norm_eps = 1e-06


MESH = pl.DeviceIdType.MESH
LANES = 128


def attention_kernel(query_ref, kv_ref, out_ref, acc_ref, later_ref):
    own = lax.axis_index("sp")
    count, width = query_ref.shape
    lane = lax.broadcasted_iota(jnp.int32, (count, LANES), 1)
    row = lax.broadcasted_iota(jnp.int32, (count, count), 0)
    column = lax.broadcasted_iota(jnp.int32, (count, count), 1)
    after = (row > column).astype(jnp.bfloat16)
    acc_ref[...] = jnp.zeros_like(acc_ref)
    later_ref[...] = jnp.zeros_like(later_ref)

    def tile(block, diagonal):
        rows = pl.ds(pl.multiple_of(block * count, count), count)
        for pair in range(width // LANES):
            columns = slice(pair * LANES, (pair + 1) * LANES)
            keys = kv_ref[rows, columns]
            values = kv_ref[rows, width + pair * LANES : width + (pair + 1) * LANES]
            sides = []
            for side in range(LANES // HEAD_DIM):
                head = pair * (LANES // HEAD_DIM) + side
                mine = (lane >= side * HEAD_DIM) & (lane < (side + 1) * HEAD_DIM)
                query = query_ref[:, columns].astype(jnp.float32) * HEAD_DIM ** (-0.5)
                query = jnp.where(mine, query, 0.0).astype(jnp.bfloat16)
                scores = lax.dot_general(
                    query, keys, (((1,), (1,)), ((), ())), preferred_element_type=jnp.float32
                )
                tail = jnp.log(1.0 + jnp.exp(-jnp.abs(scores)))
                cost = jnp.maximum(scores, 0.0) + tail
                if diagonal:
                    cost = jnp.where(column < row, cost, 0.0)
                high = cost.astype(jnp.bfloat16)
                low = (cost - high.astype(jnp.float32)).astype(jnp.bfloat16)
                inside = jnp.dot(high, after, preferred_element_type=jnp.float32)
                inside = inside + jnp.dot(low, after, preferred_element_type=jnp.float32)
                weight = jnp.exp(jnp.minimum(scores, 0.0) - tail - inside)
                if diagonal:
                    weight = jnp.where(column < row, weight, 0.0)
                partial = jnp.dot(
                    weight.astype(jnp.bfloat16), values, preferred_element_type=jnp.float32
                )
                later = later_ref[head]
                sides.append(jnp.exp(-later) * partial)
                total = inside[:, 0:1] + cost[:, 0:1]
                later_ref[head] = later + jnp.broadcast_to(total, later.shape)
            acc_ref[:, columns] += jnp.where(lane < HEAD_DIM, sides[0], sides[1])

    tile(own, True)

    def step(index, carry):
        tile(own - 1 - index, False)
        return carry

    lax.fori_loop(0, own, step, 0)
    out_ref[...] = acc_ref[...].astype(out_ref.dtype)


def attention(queries, kv):
    count, width = queries.shape
    return pl.pallas_call(
        attention_kernel,
        out_shape=jax.ShapeDtypeStruct((count, width), jnp.bfloat16),
        in_specs=[pl.BlockSpec(memory_space=pltpu.VMEM)] * 2,
        out_specs=pl.BlockSpec(memory_space=pltpu.VMEM),
        scratch_shapes=[
            pltpu.VMEM((count, width), jnp.float32),
            pltpu.VMEM((width // HEAD_DIM, count, LANES), jnp.float32),
        ],
        compiler_params=pltpu.CompilerParams(vmem_limit_bytes=56 * 1024 * 1024),
    )(queries, kv)


def gather_kernel(n, depth, in_ref, out_ref, stage, send_sem, recv_sem, local_sem):
    me = lax.axis_index("sp")
    plane = n // depth
    level, place = me // plane, lax.rem(me, plane)

    def above(k):
        return lax.rem(level + k, depth) * plane + place

    def beside(j):
        return level * plane + lax.rem(place + j, plane)

    peers = [above(k) for k in range(1, depth)] + [beside(j) for j in range(1, plane)]
    barrier = pltpu.get_barrier_semaphore()
    for peer in peers:
        pl.semaphore_signal(barrier, inc=1, device_id={"sp": peer}, device_id_type=MESH)
    pl.semaphore_wait(barrier, len(peers))

    def send(source, block, peer, k, j):
        copy = pltpu.make_async_remote_copy(
            src_ref=source,
            dst_ref=out_ref.at[block],
            send_sem=send_sem.at[k, j],
            recv_sem=recv_sem.at[k, j],
            device_id={"sp": peer},
            device_id_type=MESH,
        )
        copy.start()
        return copy

    rising = [send(in_ref, me, above(k), k, 0) for k in range(1, depth)]
    level_copies = [send(in_ref, me, beside(j), 0, j) for j in range(1, plane)]
    inward = pltpu.make_async_copy(in_ref, stage, local_sem)
    inward.start()
    inward.wait()
    outward = pltpu.make_async_copy(stage, out_ref.at[me], local_sem)
    outward.start()
    outward.wait()
    for k in range(1, depth):
        rising[k - 1].wait_recv()
        block = lax.rem(level + depth - k, depth) * plane + place
        for j in range(1, plane):
            level_copies.append(send(out_ref.at[block], block, beside(j), k, j))
    for copy in rising:
        copy.wait_send()
    for copy in level_copies:
        copy.wait()


def gather(array, n, number):
    depth = 4 if n % 4 == 0 else 1
    return pl.pallas_call(
        functools.partial(gather_kernel, n, depth),
        out_shape=jax.ShapeDtypeStruct((n,) + array.shape, array.dtype),
        in_specs=[pl.BlockSpec(memory_space=pltpu.HBM)],
        out_specs=pl.BlockSpec(memory_space=pltpu.HBM),
        scratch_shapes=[
            pltpu.VMEM(array.shape, array.dtype),
            pltpu.SemaphoreType.DMA((depth, n // depth)),
            pltpu.SemaphoreType.DMA((depth, n // depth)),
            pltpu.SemaphoreType.DMA,
        ],
        compiler_params=pltpu.CompilerParams(collective_id=number, has_side_effects=True),
    )(array)


def exchange_kernel(n, in_ref, out_ref, stage, send_sem, recv_sem, local_sem):
    me = lax.axis_index("sp")
    barrier = pltpu.get_barrier_semaphore()
    for k in range(1, n):
        pl.semaphore_signal(
            barrier, inc=1, device_id={"sp": lax.rem(me + k, n)}, device_id_type=MESH
        )
    pl.semaphore_wait(barrier, n - 1)

    def part(peer):
        return in_ref.at[peer]

    copies = []
    for k in range(1, n):
        peer = lax.rem(me + k, n)
        copy = pltpu.make_async_remote_copy(
            src_ref=part(peer),
            dst_ref=out_ref.at[me],
            send_sem=send_sem.at[k],
            recv_sem=recv_sem.at[k],
            device_id={"sp": peer},
            device_id_type=MESH,
        )
        copy.start()
        copies.append(copy)
    inward = pltpu.make_async_copy(part(me), stage, local_sem)
    inward.start()
    inward.wait()
    outward = pltpu.make_async_copy(stage, out_ref.at[me], local_sem)
    outward.start()
    outward.wait()
    for copy in copies:
        copy.wait()


def exchange(array, n, number):
    shape = array.shape[1:]
    return pl.pallas_call(
        functools.partial(exchange_kernel, n),
        out_shape=jax.ShapeDtypeStruct((n,) + shape, array.dtype),
        in_specs=[pl.BlockSpec(memory_space=pltpu.HBM)],
        out_specs=pl.BlockSpec(memory_space=pltpu.HBM),
        scratch_shapes=[
            pltpu.VMEM(shape, array.dtype),
            pltpu.SemaphoreType.DMA((n,)),
            pltpu.SemaphoreType.DMA((n,)),
            pltpu.SemaphoreType.DMA,
        ],
        compiler_params=pltpu.CompilerParams(collective_id=number, has_side_effects=True),
    )(array)


LEVELS = 4


def level_at(z, p):
    low = z * 2 < LEVELS
    place = jnp.where(low, z, LEVELS - 1 - z)
    step = jnp.where(p == 0, place, jnp.where(p - 1 < place, p - 1, p))
    return jnp.where(low, step, LEVELS - 1 - step)


def expert_kernel(
    pieces,
    normed_ref,
    mixed_ref,
    weight_ref,
    *refs,
):
    halves = [refs[3 * j : 3 * j + 3] for j in range(4)]
    shared = refs[12:15]
    out_ref = refs[15]
    (tok, acc, wg, wu, wd, sg, su, sd, shared_out, hidden, shared_hidden) = refs[16:27]
    (y_out, y_in, z_out, z_in, route) = refs[27:32]
    (load_sem, w_send, w_recv, zs_sem, zr_sem, ys_sem, yr_sem) = refs[32:39]
    (rys_sem, ryr_sem, rzs_sem, rzr_sem) = refs[39:43]
    me = lax.axis_index("sp")
    x, y, z = lax.rem(me, 2), lax.rem(me // 2, 2), me // 4
    count, width = normed_ref.shape
    experts = weight_ref.shape[0]
    half = wg.shape[2]
    rows = count // pieces

    def chip(level, side):
        return level * 4 + side * 2 + x

    loads = []
    for j in range(4):
        loads.append((halves[j][0], wg.at[j]))
        loads.append((halves[j][1], wu.at[j]))
        loads.append((halves[j][2], wd.at[pl.ds(j * half, half)]))
    loads = list(zip(shared, (sg, su, sd))) + loads
    loads = [
        pltpu.make_async_copy(source, target, load_sem.at[k])
        for k, (source, target) in enumerate(loads)
    ]
    for load in loads:
        load.start()

    barrier = pltpu.get_barrier_semaphore()
    peers = [(dz, r) for dz in range(LEVELS) for r in range(2) if (dz, r) != (0, 0)]
    for dz, r in peers:
        peer = chip(lax.rem(z + dz, LEVELS), lax.rem(y + r, 2))
        pl.semaphore_signal(barrier, inc=1, device_id={"sp": peer}, device_id_type=MESH)
    pl.semaphore_wait(barrier, len(peers))

    def remote(source, target, send, recv, peer):
        return pltpu.make_async_remote_copy(
            src_ref=source,
            dst_ref=target,
            send_sem=send,
            recv_sem=recv,
            device_id={"sp": peer},
            device_id_type=MESH,
        )

    def part(c):
        return pl.ds(c * rows, rows)

    beside = chip(z, 1 - y)
    above, below = me + 4, me - 4

    def along(source, t, c, up):
        return remote(
            source,
            tok.at[t, 0, part(c)],
            zs_sem.at[0 if up else 1, t, c],
            zr_sem.at[t, c],
            above if up else below,
        )

    def across(source, t, c):
        return remote(
            source, tok.at[t, 1, part(c)], ys_sem.at[t, c], yr_sem.at[t, c], beside
        )

    def spread(source, t, c):
        @pl.when((t <= z) & (z < LEVELS - 1))
        def _():
            along(source, t, c, True).start()

        @pl.when((t >= z) & (z > 0))
        def _():
            along(source, t, c, False).start()

        across(source, t, c).start()

    for c in range(pieces):
        spread(normed_ref.at[part(c)], z, c)

    def route_copy(dz, r, incoming):
        origin = lax.rem(z + LEVELS - dz, LEVELS) if incoming else z
        peer = chip(lax.rem(z + dz, LEVELS), lax.rem(y + r, 2))
        return remote(
            weight_ref, route.at[origin * 2 + r], w_send.at[dz, r], w_recv.at[dz, r], peer
        )

    for dz, r in peers:
        route_copy(dz, r, False).start()
    route[z * 2] = weight_ref[...]
    tok[z, 0] = normed_ref[...]

    for load in loads[:3]:
        load.wait()
    span = min(width, 512)
    shared_half = sg.shape[1] // 2
    for j in range(2):
        columns = slice(j * shared_half, (j + 1) * shared_half)
        gate = jnp.dot(normed_ref[...], sg[:, columns], preferred_element_type=jnp.float32)
        upward = jnp.dot(normed_ref[...], su[:, columns], preferred_element_type=jnp.float32)
        shared_hidden[:, columns] = (jax.nn.silu(gate) * upward).astype(jnp.bfloat16)

    def shared_step(k, carry):
        columns = pl.ds(pl.multiple_of(k * span, span), span)
        shared_out[:, columns] = mixed_ref[:, columns].astype(jnp.float32) + jnp.dot(
            shared_hidden[...], sd[:, columns], preferred_element_type=jnp.float32
        )
        return carry

    lax.fori_loop(0, width // span, shared_step, 0)

    for dz, r in peers:
        route_copy(dz, r, True).wait_recv()
    for load in loads[3:]:
        load.wait()

    def forward(p):
        t = level_at(z, p)
        for c in range(pieces):
            remote(
                normed_ref.at[part(c)], tok.at[t, 0, part(c)], zs_sem.at[0, t, c],
                zr_sem.at[t, c], beside,
            ).wait_recv()
            spread(tok.at[t, 0, part(c)], t, c)

    lane = lax.broadcasted_iota(jnp.int32, (count, LANES), 1)

    def column(slot, expert):
        table = jnp.concatenate(
            [route[slot], jnp.zeros((LANES - experts, count), jnp.float32)], axis=0
        )
        picked = jnp.where(lane == expert, jnp.transpose(table), 0.0)
        return jnp.sum(picked, axis=1, keepdims=True)

    def give(t):
        for c in range(pieces):
            remote(
                y_out.at[t, part(c)], y_in.at[t, part(c)], rys_sem.at[t, c],
                ryr_sem.at[t, c], beside,
            ).start()

    def step(i, carry):
        @pl.when(i == 0)
        def _():
            forward(1)
            forward(2)

        @pl.when(i == 1)
        def _():
            forward(3)

        t = level_at(z, i)
        for c in range(pieces):
            across(normed_ref.at[part(c)], t, c).wait_recv()
        sides = [
            jnp.concatenate([column(t * 2, e), column(t * 2 + 1, e)], axis=0)
            for e in (me, me + 1 - 2 * x)
        ]

        def inner(j, carry):
            block = tok[t].reshape(2 * count, width)
            gate = jnp.dot(block, wg[j], preferred_element_type=jnp.float32)
            upward = jnp.dot(block, wu[j], preferred_element_type=jnp.float32)
            scale = jnp.where(j < 2, sides[0], sides[1])
            columns = pl.ds(pl.multiple_of(j * half, half), half)
            hidden[:, columns] = (jax.nn.silu(gate) * upward * scale).astype(jnp.bfloat16)
            return carry

        lax.fori_loop(0, 4, inner, 0)

        def outer(k, carry):
            columns = pl.ds(pl.multiple_of(k * span, span), span)
            result = jnp.dot(hidden[...], wd[:, columns], preferred_element_type=jnp.float32)
            acc[t, :, columns] = result[:count]
            y_out[t, :, columns] = result[count:].astype(jnp.bfloat16)
            return carry

        lax.fori_loop(0, width // span, outer, 0)

        @pl.when(i == 2)
        def _():
            give(level_at(z, 2))

        @pl.when(i == 3)
        def _():
            give(level_at(z, 3))
            give(level_at(z, 1))
            give(level_at(z, 0))

        return carry

    lax.fori_loop(0, LEVELS, step, 0)

    def take(t, c):
        remote(
            y_out.at[t, part(c)], y_in.at[t, part(c)], rys_sem.at[t, c],
            ryr_sem.at[t, c], beside,
        ).wait_recv()

    def arrive(slot, c):
        remote(
            z_out.at[0, part(c)], z_in.at[slot, part(c)], rzs_sem.at[0, c],
            rzr_sem.at[slot, c], beside,
        ).wait_recv()

    def hop(p, c):
        t = level_at(z, p)
        up = t > z
        slot = jnp.where(up | (t < z - 1), t, LEVELS)
        return remote(
            z_out.at[t, part(c)],
            z_in.at[slot, part(c)],
            rzs_sem.at[t, c],
            rzr_sem.at[slot, c],
            jnp.where(up, above, below),
        )

    for p in (2, 3, 1):
        t = level_at(z, p)
        up = t > z
        fed = (up & (z > 0)) | (jnp.logical_not(up) & (z < LEVELS - 1))
        for c in range(pieces):
            take(t, c)

            @pl.when(fed)
            def _():
                arrive(t, c)
                z_out[t, part(c)] = (
                    acc[t, part(c)]
                    + y_in[t, part(c)].astype(jnp.float32)
                    + z_in[t, part(c)].astype(jnp.float32)
                ).astype(jnp.bfloat16)

            @pl.when(jnp.logical_not(fed))
            def _():
                z_out[t, part(c)] = (
                    acc[t, part(c)] + y_in[t, part(c)].astype(jnp.float32)
                ).astype(jnp.bfloat16)

            hop(p, c).start()

    for c in range(pieces):
        shared_out[part(c)] += acc[z, part(c)]

        @pl.when(z > 0)
        def _():
            arrive(z, c)
            shared_out[part(c)] += z_in[z, part(c)].astype(jnp.float32)

        @pl.when(z < LEVELS - 1)
        def _():
            arrive(LEVELS, c)
            shared_out[part(c)] += z_in[LEVELS, part(c)].astype(jnp.float32)

        take(z, c)
        out_ref[part(c)] = (
            shared_out[part(c)] + y_in[z, part(c)].astype(jnp.float32)
        ).astype(out_ref.dtype)

    for dz, r in peers:
        route_copy(dz, r, False).wait_send()

    def drain(t, carry):
        for c in range(pieces):
            @pl.when((t <= z) & (z < LEVELS - 1))
            def _():
                along(tok.at[t, 0, part(c)], t, c, True).wait_send()

            @pl.when((t >= z) & (z > 0))
            def _():
                along(tok.at[t, 0, part(c)], t, c, False).wait_send()

            across(tok.at[t, 0, part(c)], t, c).wait_send()
            remote(
                y_out.at[t, part(c)], y_in.at[t, part(c)], rys_sem.at[t, c],
                ryr_sem.at[t, c], beside,
            ).wait_send()
        return carry

    lax.fori_loop(0, LEVELS, drain, 0)
    for p in (1, 2, 3):
        for c in range(pieces):
            hop(p, c).wait_send()


def expert_layer(normed, mixed, weights, halves, shared, number):
    count, width = normed.shape
    half = halves[0][0].shape[1]
    middle = shared[0].shape[1]
    pieces = 4
    flat = [array for trio in halves for array in trio] + list(shared)
    vmem, hbm = pl.BlockSpec(memory_space=pltpu.VMEM), pl.BlockSpec(memory_space=pl.ANY)
    bf16, f32 = jnp.bfloat16, jnp.float32
    dma = pltpu.SemaphoreType.DMA
    return pl.pallas_call(
        functools.partial(expert_kernel, pieces),
        out_shape=jax.ShapeDtypeStruct((count, width), bf16),
        in_specs=[vmem] * 3 + [hbm] * len(flat),
        out_specs=vmem,
        scratch_shapes=[
            pltpu.VMEM((LEVELS, 2, count, width), bf16),
            pltpu.VMEM((LEVELS, count, width), f32),
            pltpu.VMEM((4, width, half), bf16),
            pltpu.VMEM((4, width, half), bf16),
            pltpu.VMEM((4 * half, width), bf16),
            pltpu.VMEM((width, middle), bf16),
            pltpu.VMEM((width, middle), bf16),
            pltpu.VMEM((middle, width), bf16),
            pltpu.VMEM((count, width), f32),
            pltpu.VMEM((2 * count, 4 * half), bf16),
            pltpu.VMEM((count, middle), bf16),
            pltpu.VMEM((LEVELS, count, width), bf16),
            pltpu.VMEM((LEVELS, count, width), bf16),
            pltpu.VMEM((LEVELS, count, width), bf16),
            pltpu.VMEM((LEVELS + 1, count, width), bf16),
            pltpu.VMEM((2 * LEVELS,) + weights.shape, f32),
            dma((len(flat),)),
            dma((LEVELS, 2)),
            dma((LEVELS, 2)),
            dma((2, LEVELS, pieces)),
            dma((LEVELS, pieces)),
            dma((LEVELS, pieces)),
            dma((LEVELS, pieces)),
            dma((LEVELS, pieces)),
            dma((LEVELS, pieces)),
            dma((LEVELS, pieces)),
            dma((LEVELS + 1, pieces)),
        ],
        compiler_params=pltpu.CompilerParams(
            collective_id=number,
            has_side_effects=True,
            vmem_limit_bytes=60 * 1024 * 1024,
        ),
    )(normed, mixed, weights, *flat)


def swapped(array, axis, size):
    return lax.ppermute(array, axis, [(i, i ^ 1) for i in range(size)])


def expert_product(rows, gate_half, up_half, down_half):
    gate = jnp.einsum("seid,edf->seif", rows, gate_half, preferred_element_type=jnp.float32)
    upward = jnp.einsum("seid,edf->seif", rows, up_half, preferred_element_type=jnp.float32)
    hidden = (jax.nn.silu(gate) * upward).astype(jnp.bfloat16)
    return jnp.einsum("seif,efd->seid", hidden, down_half, preferred_element_type=jnp.float32)


def local(
    queries,
    key_rows,
    value_rows,
    residual,
    out_weight,
    norm_gain,
    routes,
    route_weight,
    expert_gate,
    expert_up,
    expert_down,
    shared_gate,
    shared_up,
    shared_down,
):
    query_count = queries.shape[0]
    local_width = queries.shape[1]
    blocks = lax.axis_size("sp")
    kv = jnp.concatenate([key_rows, value_rows], axis=1)
    kv = gather(kv, blocks, 0).reshape(-1, kv.shape[1])
    attended = attention(queries, kv)
    token_rows = residual.shape[0]
    weight_rows = lax.dynamic_slice_in_dim(
        out_weight, lax.axis_index("tp") * local_width, local_width, 0
    )
    projected = lax.psum_scatter(
        jnp.dot(attended, weight_rows, preferred_element_type=jnp.float32),
        "tp",
        scatter_dimension=0,
        tiled=True,
    )
    mixed_wide = (residual.astype(jnp.float32) + projected).astype(jnp.bfloat16).astype(jnp.float32)
    inverse = lax.rsqrt(jnp.mean(mixed_wide * mixed_wide, axis=1, keepdims=True) + norm_eps)
    normed = (mixed_wide * inverse * norm_gain).astype(jnp.bfloat16)
    width = normed.shape[1]
    local_experts = expert_gate.shape[0]
    experts_all = blocks * local_experts
    if blocks == 4 * LEVELS and local_experts == 1 and lax.axis_size("tp") == 2:
        own = [expert_gate[0], expert_up[0], expert_down[0]]
        other = [swapped(array, "tp", 2) for array in own]
        near = [swapped(array, "sp", blocks) for array in own]
        far = [swapped(array, "tp", 2) for array in near]
        picked = routes[:, :, None] == jnp.arange(experts_all, dtype=jnp.int32)
        table = jnp.sum(jnp.where(picked, route_weight[:, :, None], 0.0), axis=1)
        return expert_layer(
            normed,
            mixed_wide.astype(jnp.bfloat16),
            table.T,
            (own, other, near, far),
            (shared_gate, shared_up, shared_down),
            1,
        )
    capacity = max(2, token_rows * TOPK * 5 // (4 * experts_all))
    flat_routes = routes.reshape(-1)
    picks = (flat_routes[:, None] == jnp.arange(experts_all, dtype=jnp.int32)[None, :]).astype(
        jnp.int32
    )
    earlier = jnp.cumsum(picks, axis=0) - picks
    position = flat_routes * capacity + jnp.sum(earlier * picks, axis=1)
    filler = (
        jnp.zeros((experts_all * capacity,), jnp.int32)
        .at[position]
        .set(jnp.arange(flat_routes.shape[0], dtype=jnp.int32) + 1)
    )
    occupied = filler > 0
    source_token = jnp.maximum(filler - 1, 0) // TOPK
    outgoing = jnp.where(
        occupied[:, None], normed[source_token], jnp.zeros((), jnp.bfloat16)
    ).reshape(experts_all, capacity, width)
    both = lax.all_gather(
        exchange(
            outgoing.reshape(blocks, local_experts * capacity, width), blocks, 1
        ).reshape(outgoing.shape),
        "tp",
        axis=0,
        tiled=True,
    )
    shaped = both.reshape(-1, local_experts, both.shape[1], both.shape[2])
    pieces = expert_product(shaped, expert_gate, expert_up, expert_down).reshape(both.shape)
    summed = lax.psum_scatter(pieces.astype(jnp.bfloat16), "tp", scatter_dimension=0, tiled=True)
    results = exchange(
        summed.reshape(blocks, local_experts * capacity, width), blocks, 2
    ).reshape(
        experts_all * capacity, width
    )
    picked = results[position].reshape(token_rows, TOPK, width)
    routed = jnp.sum(picked.astype(jnp.float32) * route_weight[:, :, None], axis=1)
    shared_gate_out = jnp.dot(normed, shared_gate, preferred_element_type=jnp.float32)
    shared_up_out = jnp.dot(normed, shared_up, preferred_element_type=jnp.float32)
    shared_act = (jax.nn.silu(shared_gate_out) * shared_up_out).astype(jnp.bfloat16)
    shared_out = jnp.dot(shared_act, shared_down, preferred_element_type=jnp.float32)
    return (mixed_wide + routed + shared_out).astype(jnp.bfloat16)


def solution(mesh):
    return jax.shard_map(
        local,
        mesh=mesh,
        in_specs=(
            P("sp", "tp"),
            P("sp", "tp"),
            P("sp", "tp"),
            P(("sp", "tp"), None),
            P(),
            P(),
            P(("sp", "tp"), None),
            P(("sp", "tp"), None),
            P("sp", None, "tp"),
            P("sp", None, "tp"),
            P("sp", "tp", None),
            P(),
            P(),
            P(),
        ),
        out_specs=P(("sp", "tp"), None),
        check_vma=False,
    )
```

```python
import functools

import jax
import jax.numpy as jnp
from jax import lax
from jax.experimental import pallas as pl
from jax.experimental.pallas import tpu as pltpu
from jax.sharding import PartitionSpec as P

HEAD_DIM = 64
TOPK = 8


norm_eps = 1e-06


MESH = pl.DeviceIdType.MESH
LANES = 128


def attention_kernel(query_ref, kv_ref, out_ref, acc_ref, later_ref):
    own = lax.axis_index("sp")
    count, width = query_ref.shape
    lane = lax.broadcasted_iota(jnp.int32, (count, LANES), 1)
    row = lax.broadcasted_iota(jnp.int32, (count, count), 0)
    column = lax.broadcasted_iota(jnp.int32, (count, count), 1)
    after = (row > column).astype(jnp.bfloat16)
    acc_ref[...] = jnp.zeros_like(acc_ref)
    later_ref[...] = jnp.zeros_like(later_ref)

    def tile(block, diagonal):
        rows = pl.ds(pl.multiple_of(block * count, count), count)
        for pair in range(width // LANES):
            columns = slice(pair * LANES, (pair + 1) * LANES)
            keys = kv_ref[rows, columns]
            values = kv_ref[rows, width + pair * LANES : width + (pair + 1) * LANES]
            sides = []
            for side in range(LANES // HEAD_DIM):
                head = pair * (LANES // HEAD_DIM) + side
                mine = (lane >= side * HEAD_DIM) & (lane < (side + 1) * HEAD_DIM)
                query = query_ref[:, columns].astype(jnp.float32) * HEAD_DIM ** (-0.5)
                query = jnp.where(mine, query, 0.0).astype(jnp.bfloat16)
                scores = lax.dot_general(
                    query, keys, (((1,), (1,)), ((), ())), preferred_element_type=jnp.float32
                )
                tail = jnp.log(1.0 + jnp.exp(-jnp.abs(scores)))
                cost = jnp.maximum(scores, 0.0) + tail
                if diagonal:
                    cost = jnp.where(column < row, cost, 0.0)
                high = cost.astype(jnp.bfloat16)
                low = (cost - high.astype(jnp.float32)).astype(jnp.bfloat16)
                inside = jnp.dot(high, after, preferred_element_type=jnp.float32)
                inside = inside + jnp.dot(low, after, preferred_element_type=jnp.float32)
                weight = jnp.exp(jnp.minimum(scores, 0.0) - tail - inside)
                if diagonal:
                    weight = jnp.where(column < row, weight, 0.0)
                partial = jnp.dot(
                    weight.astype(jnp.bfloat16), values, preferred_element_type=jnp.float32
                )
                later = later_ref[head]
                sides.append(jnp.exp(-later) * partial)
                total = inside[:, 0:1] + cost[:, 0:1]
                later_ref[head] = later + jnp.broadcast_to(total, later.shape)
            acc_ref[:, columns] += jnp.where(lane < HEAD_DIM, sides[0], sides[1])

    tile(own, True)

    def step(index, carry):
        tile(own - 1 - index, False)
        return carry

    lax.fori_loop(0, own, step, 0)
    out_ref[...] = acc_ref[...].astype(out_ref.dtype)


def attention(queries, kv):
    count, width = queries.shape
    return pl.pallas_call(
        attention_kernel,
        out_shape=jax.ShapeDtypeStruct((count, width), jnp.bfloat16),
        in_specs=[pl.BlockSpec(memory_space=pltpu.VMEM)] * 2,
        out_specs=pl.BlockSpec(memory_space=pltpu.VMEM),
        scratch_shapes=[
            pltpu.VMEM((count, width), jnp.float32),
            pltpu.VMEM((width // HEAD_DIM, count, LANES), jnp.float32),
        ],
        compiler_params=pltpu.CompilerParams(vmem_limit_bytes=56 * 1024 * 1024),
    )(queries, kv)


def gather_kernel(n, depth, in_ref, out_ref, stage, send_sem, recv_sem, local_sem):
    me = lax.axis_index("sp")
    plane = n // depth
    level, place = me // plane, lax.rem(me, plane)

    def above(k):
        return lax.rem(level + k, depth) * plane + place

    def beside(j):
        return level * plane + lax.rem(place + j, plane)

    peers = [above(k) for k in range(1, depth)] + [beside(j) for j in range(1, plane)]
    barrier = pltpu.get_barrier_semaphore()
    for peer in peers:
        pl.semaphore_signal(barrier, inc=1, device_id={"sp": peer}, device_id_type=MESH)
    pl.semaphore_wait(barrier, len(peers))

    def send(source, block, peer, k, j):
        copy = pltpu.make_async_remote_copy(
            src_ref=source,
            dst_ref=out_ref.at[block],
            send_sem=send_sem.at[k, j],
            recv_sem=recv_sem.at[k, j],
            device_id={"sp": peer},
            device_id_type=MESH,
        )
        copy.start()
        return copy

    rising = [send(in_ref, me, above(k), k, 0) for k in range(1, depth)]
    level_copies = [send(in_ref, me, beside(j), 0, j) for j in range(1, plane)]
    inward = pltpu.make_async_copy(in_ref, stage, local_sem)
    inward.start()
    inward.wait()
    outward = pltpu.make_async_copy(stage, out_ref.at[me], local_sem)
    outward.start()
    outward.wait()
    for k in range(1, depth):
        rising[k - 1].wait_recv()
        block = lax.rem(level + depth - k, depth) * plane + place
        for j in range(1, plane):
            level_copies.append(send(out_ref.at[block], block, beside(j), k, j))
    for copy in rising:
        copy.wait_send()
    for copy in level_copies:
        copy.wait()


def gather(array, n, number):
    depth = 4 if n % 4 == 0 else 1
    return pl.pallas_call(
        functools.partial(gather_kernel, n, depth),
        out_shape=jax.ShapeDtypeStruct((n,) + array.shape, array.dtype),
        in_specs=[pl.BlockSpec(memory_space=pltpu.HBM)],
        out_specs=pl.BlockSpec(memory_space=pltpu.HBM),
        scratch_shapes=[
            pltpu.VMEM(array.shape, array.dtype),
            pltpu.SemaphoreType.DMA((depth, n // depth)),
            pltpu.SemaphoreType.DMA((depth, n // depth)),
            pltpu.SemaphoreType.DMA,
        ],
        compiler_params=pltpu.CompilerParams(collective_id=number, has_side_effects=True),
    )(array)


def exchange_kernel(n, in_ref, out_ref, stage, send_sem, recv_sem, local_sem):
    me = lax.axis_index("sp")
    barrier = pltpu.get_barrier_semaphore()
    for k in range(1, n):
        pl.semaphore_signal(
            barrier, inc=1, device_id={"sp": lax.rem(me + k, n)}, device_id_type=MESH
        )
    pl.semaphore_wait(barrier, n - 1)

    def part(peer):
        return in_ref.at[peer]

    copies = []
    for k in range(1, n):
        peer = lax.rem(me + k, n)
        copy = pltpu.make_async_remote_copy(
            src_ref=part(peer),
            dst_ref=out_ref.at[me],
            send_sem=send_sem.at[k],
            recv_sem=recv_sem.at[k],
            device_id={"sp": peer},
            device_id_type=MESH,
        )
        copy.start()
        copies.append(copy)
    inward = pltpu.make_async_copy(part(me), stage, local_sem)
    inward.start()
    inward.wait()
    outward = pltpu.make_async_copy(stage, out_ref.at[me], local_sem)
    outward.start()
    outward.wait()
    for copy in copies:
        copy.wait()


def exchange(array, n, number):
    shape = array.shape[1:]
    return pl.pallas_call(
        functools.partial(exchange_kernel, n),
        out_shape=jax.ShapeDtypeStruct((n,) + shape, array.dtype),
        in_specs=[pl.BlockSpec(memory_space=pltpu.HBM)],
        out_specs=pl.BlockSpec(memory_space=pltpu.HBM),
        scratch_shapes=[
            pltpu.VMEM(shape, array.dtype),
            pltpu.SemaphoreType.DMA((n,)),
            pltpu.SemaphoreType.DMA((n,)),
            pltpu.SemaphoreType.DMA,
        ],
        compiler_params=pltpu.CompilerParams(collective_id=number, has_side_effects=True),
    )(array)


LEVELS = 4
WEIGHT_CUTS = 4


def level_at(z, p):
    low = z * 2 < LEVELS
    place = jnp.where(low, z, LEVELS - 1 - z)
    step = jnp.where(p == 0, place, jnp.where(p - 1 < place, p - 1, p))
    return jnp.where(low, step, LEVELS - 1 - step)


def layer_kernel(pieces, names, *refs):
    s = dict(zip(names, refs))
    f32, bf16 = jnp.float32, jnp.bfloat16
    me, core = lax.axis_index("sp"), lax.axis_index("tp")
    x, y, z = lax.rem(me, 2), lax.rem(me // 2, 2), me // 4
    out_ref = s["out"]
    count, width = out_ref.shape
    tokens = s["query"].shape[0]
    blocks = s["kv"].shape[0]
    experts = s["table"].shape[0]
    half = s["wg"].shape[2]
    rows = count // pieces
    span = min(width, 512)

    def chip(level, side, place):
        return level * 4 + side * 2 + place

    def remote(source, target, send, recv, peer, peer_core=None):
        return pltpu.make_async_remote_copy(
            src_ref=source,
            dst_ref=target,
            send_sem=send,
            recv_sem=recv,
            device_id={"sp": peer, "tp": core if peer_core is None else peer_core},
            device_id_type=MESH,
        )

    pair = me + 1 - 2 * x
    beside = chip(z, 1 - y, x)
    above, below = me + 4, me - 4
    mirror = chip(LEVELS - 1 - z, 1 - y, 0)

    def landed(target, recv):
        remote(target, target, s["idle"].at[0], recv, beside).wait_recv()

    wg, wu, wd = s["wg"], s["wu"], s["wd"]

    def trio(j):
        return wg.at[j], wu.at[j], wd.at[pl.ds(j * half, half)]

    loads = list(zip((s["gate"], s["up"], s["down"]), trio(0)))
    loads += [(s["project"], s["wo"])]
    loads += list(zip((s["shared_gate"], s["shared_up"], s["shared_down"]), (s["sg"], s["su"], s["sd"])))
    loads = [
        pltpu.make_async_copy(source, target, s["load_sem"].at[k])
        for k, (source, target) in enumerate(loads)
    ]
    for load in loads:
        load.start()

    def lanes(place):
        return pl.ds(pl.multiple_of(place * LANES, LANES), LANES)

    kv = s["kv"]
    near = [
        pltpu.make_async_copy(s[name].at[:, lanes(x)], kv.at[me, k], s["near_sem"].at[k])
        for k, name in enumerate(("key", "value"))
    ]
    for copy in near:
        copy.start()

    barrier = pltpu.get_barrier_semaphore()
    peers = [(dz, r) for dz in range(LEVELS) for r in range(2) if (dz, r) != (0, 0)]
    greeted = [
        (chip(lax.rem(z + dz, LEVELS), lax.rem(y + r, 2), x), core) for dz, r in peers
    ]
    greeted += [(me, 1 - core), (pair, core), (pair, 1 - core)]
    greeted += [(mirror + x, 1 - core), (mirror + 1 - x, core), (mirror + 1 - x, 1 - core)]
    for peer, peer_core in greeted:
        pl.semaphore_signal(
            barrier, inc=1, device_id={"sp": peer, "tp": peer_core}, device_id_type=MESH
        )
    pl.semaphore_wait(barrier, len(greeted))

    swaps = [
        remote(
            s[name].at[:, lanes(1 - x)], kv.at[me, k], s["kxs"].at[k], s["kxr"].at[k], pair
        )
        for k, name in enumerate(("key", "value"))
    ]
    for copy in swaps:
        copy.start()

    query, qs = s["query"], s["qs"]
    kept = pltpu.make_async_copy(query.at[:, lanes(0)], qs.at[0], s["near_sem"].at[2])

    def query_send(place):
        keep = remote(
            query.at[:, lanes(1)], qs.at[0], s["qss"].at[1], s["qsr"].at[0], pair
        )
        move = remote(
            query.at[:, lanes(place)], qs.at[1], s["qss"].at[place], s["qsr"].at[1],
            mirror + place,
        )
        return keep, move

    @pl.when(x == 0)
    def _():
        kept.start()
        query_send(1)[0].start()

    @pl.when(x == 1)
    def _():
        query_send(0)[1].start()
        query_send(1)[1].start()

    def kv_along(b, up):
        return remote(
            kv.at[b], kv.at[b], s["kzs"].at[0 if up else 1, b], s["kzr"].at[b],
            above if up else below,
        )

    def kv_across(b):
        return remote(kv.at[b], kv.at[b], s["kys"].at[b], s["kyr"].at[b], beside)

    def kv_spread(b):
        t = b // 4

        @pl.when((t <= z) & (z < LEVELS - 1))
        def _():
            kv_along(b, True).start()

        @pl.when((t >= z) & (z > 0))
        def _():
            kv_along(b, False).start()

        kv_across(b).start()

    for copy in near:
        copy.wait()
    kv_spread(me)

    def route_copy(dz, r, incoming):
        origin = lax.rem(z + LEVELS - dz, LEVELS) if incoming else z
        peer = chip(lax.rem(z + dz, LEVELS), lax.rem(y + r, 2), x)
        return remote(
            s["table"], s["route"].at[origin * 2 + r], s["w_send"].at[dz, r],
            s["w_recv"].at[dz, r], peer,
        )

    for dz, r in peers:
        route_copy(dz, r, False).start()
    s["route"][z * 2] = s["table"][...]

    for load in loads[:3]:
        load.wait()

    def core_copy(j, a):
        k = 3 * (j // 2) + a
        return remote(
            trio(j)[a], trio(j + 1)[a], s["wts"].at[k], s["wtr"].at[k], me, 1 - core
        )

    def weight_piece(k):
        a, r = k // WEIGHT_CUTS, k % WEIGHT_CUTS
        source, target = trio(0)[a], trio(2)[a]
        size = source.shape[0] // WEIGHT_CUTS
        cut = pl.ds(r * size, size)
        return remote(source.at[cut], target.at[cut], s["wxs"].at[k], s["wxr"].at[k], pair)

    for a in range(3):
        core_copy(0, a).start()
    for k in range(2):
        weight_piece(k).start()

    row = lax.broadcasted_iota(jnp.int32, (tokens, tokens), 0)
    column = lax.broadcasted_iota(jnp.int32, (tokens, tokens), 1)
    s["after"][...] = (row > column).astype(bf16)
    s["seg"][...] = jnp.zeros_like(s["seg"])
    s["sum"][...] = jnp.zeros_like(s["sum"])

    for k in range(2):
        landed(kv.at[pair, k], s["kxr"].at[k])
    kv_spread(pair)

    @pl.when(x == 0)
    def _():
        kept.wait()

    @pl.when(x == 1)
    def _():
        landed(qs.at[0], s["qsr"].at[0])

    landed(qs.at[1], s["qsr"].at[1])
    lane = lax.broadcasted_iota(jnp.int32, (tokens, LANES), 1)
    first = lane < HEAD_DIM
    for f in range(2):
        scaled = qs[f].astype(f32) * HEAD_DIM ** (-0.5)
        s["qm"][f, 0] = jnp.where(first, scaled, 0.0).astype(bf16)
        s["qm"][f, 1] = jnp.where(first, 0.0, scaled).astype(bf16)

    def kv_forward(p):
        t = level_at(z, p)
        for k in range(2):
            b = chip(t, y, k)
            landed(kv.at[b], s["kzr"].at[b])
            kv_spread(b)

    def tile(f, t, b, diagonal):
        parts, totals = [], []
        for h in range(2):
            scores = lax.dot_general(
                s["qm"][f, h], kv[b, 0], (((1,), (1,)), ((), ())), preferred_element_type=f32
            )
            tail = jnp.log(1.0 + jnp.exp(-jnp.abs(scores)))
            cost = jnp.maximum(scores, 0.0) + tail
            if diagonal:
                mask = lax.broadcasted_iota(
                    jnp.int32, (tokens, tokens), 1
                ) < lax.broadcasted_iota(jnp.int32, (tokens, tokens), 0)
                cost = jnp.where(mask, cost, 0.0)
            high = cost.astype(bf16)
            low = (cost - high.astype(f32)).astype(bf16)
            inside = jnp.dot(high, s["after"][...], preferred_element_type=f32)
            inside = inside + jnp.dot(low, s["after"][...], preferred_element_type=f32)
            weight = jnp.exp(jnp.minimum(scores, 0.0) - tail - inside)
            if diagonal:
                weight = jnp.where(mask, weight, 0.0)
            parts.append(jnp.dot(weight.astype(bf16), kv[b, 1], preferred_element_type=f32))
            totals.append(inside[:, 0:1] + cost[:, 0:1])
        total = jnp.where(first, totals[0], totals[1])
        s["seg"][f, t] = s["seg"][f, t] * jnp.exp(-total) + jnp.where(first, parts[0], parts[1])
        s["sum"][f, t] += total

    kept_block = chip(z, y, 0)

    def attend(i, carry):
        @pl.when(i == 0)
        def _():
            kv_forward(1)
            kv_forward(2)

        @pl.when(i == 1)
        def _():
            kv_forward(3)

        t = level_at(z, i)
        for k in range(2):
            b = chip(t, 1 - y, k)
            landed(kv.at[b], s["kyr"].at[b])

        def one_query(f, carry):
            block = jnp.where(f == 0, kept_block, blocks - 1 - kept_block)
            full = jnp.clip(block - 4 * t, 0, 4)

            def one_key(b, carry):
                tile(f, t, 4 * t + b, False)
                return carry

            lax.fori_loop(0, full, one_key, 0)

            @pl.when((block >= 4 * t) & (block < 4 * t + 4))
            def _():
                tile(f, t, block, True)

            return carry

        lax.fori_loop(0, 2, one_query, 0)

        @pl.when(i == 0)
        def _():
            weight_piece(2).start()
            weight_piece(3).start()

        @pl.when(i == 1)
        def _():
            weight_piece(4).start()

        @pl.when(i == 2)
        def _():
            weight_piece(5).start()

        return carry

    lax.fori_loop(0, LEVELS, attend, 0)

    for f in range(2):
        later = s["sum"][f, LEVELS - 1]
        value = s["seg"][f, LEVELS - 1]
        for t in reversed(range(LEVELS - 1)):
            value = value + jnp.exp(-later) * s["seg"][f, t]
            later = later + s["sum"][f, t]
        s["ob"][f] = value.astype(bf16)

    spot = core * 2 + x

    def attended_copy(f, d):
        other = lax.rem(core + d, 2)
        source = s["ob"].at[f, pl.ds(pl.multiple_of(other * count, count), count)]
        target = kept_block if f == 0 else mirror + 1
        return remote(
            source, s["att"].at[spot], s["oss"].at[f, d], s["osr"].at[spot], target, other
        )

    attended_copy(1, 0).start()
    attended_copy(1, 1).start()
    attended_copy(0, 1).start()

    @pl.when(x == 1)
    def _():
        attended_copy(0, 0).start()

    @pl.when(x == 0)
    def _():
        s["att"][spot] = s["ob"][0, pl.ds(pl.multiple_of(core * count, count), count)]

    loads[3].wait()
    for k in range(4):
        @pl.when((x == 1) | (k != spot))
        def _():
            landed(s["att"].at[k], s["osr"].at[k])

    for k in range(6, 3 * WEIGHT_CUTS):
        weight_piece(k).start()

    mixed, normed = s["mixed"], s["normed"]
    attended = jnp.concatenate([s["att"][k] for k in range(4)], axis=1)

    def project_step(k, carry):
        columns = pl.ds(pl.multiple_of(k * span, span), span)
        value = s["residual"][:, columns].astype(f32) + jnp.dot(
            attended, s["wo"][:, columns], preferred_element_type=f32
        )
        value = value.astype(bf16)
        mixed[:, columns] = value
        value = value.astype(f32)
        return carry + jnp.sum(value * value, axis=1, keepdims=True)

    squares = lax.fori_loop(0, width // span, project_step, jnp.zeros((count, 1), f32))
    inverse = lax.rsqrt(squares / width + norm_eps)
    for k in range(width // span):
        columns = slice(k * span, (k + 1) * span)
        normed[:, columns] = (
            mixed[:, columns].astype(f32) * inverse * s["gain"][:, columns]
        ).astype(bf16)

    tok, acc = s["tok"], s["acc"]
    y_out, y_in, z_out, z_in = s["y_out"], s["y_in"], s["z_out"], s["z_in"]

    def part(c):
        return pl.ds(c * rows, rows)

    def along(source, t, c, up):
        return remote(
            source,
            tok.at[t, 0, part(c)],
            s["zs"].at[0 if up else 1, t, c],
            s["zr"].at[t, c],
            above if up else below,
        )

    def across(source, t, c):
        return remote(
            source, tok.at[t, 1, part(c)], s["ys"].at[t, c], s["yr"].at[t, c], beside
        )

    def spread(source, t, c):
        @pl.when((t <= z) & (z < LEVELS - 1))
        def _():
            along(source, t, c, True).start()

        @pl.when((t >= z) & (z > 0))
        def _():
            along(source, t, c, False).start()

        across(source, t, c).start()

    tok[z, 0] = normed[...]
    for c in range(pieces):
        spread(normed.at[part(c)], z, c)

    for load in loads[4:]:
        load.wait()
    shared_out = s["shared_out"]
    shared_half = s["sg"].shape[1] // 2
    for j in range(2):
        columns = slice(j * shared_half, (j + 1) * shared_half)
        gate = jnp.dot(normed[...], s["sg"][:, columns], preferred_element_type=f32)
        upward = jnp.dot(normed[...], s["su"][:, columns], preferred_element_type=f32)
        s["shared_hidden"][:, columns] = (jax.nn.silu(gate) * upward).astype(bf16)

    def shared_step(k, carry):
        columns = pl.ds(pl.multiple_of(k * span, span), span)
        shared_out[:, columns] = mixed[:, columns].astype(f32) + jnp.dot(
            s["shared_hidden"][...], s["sd"][:, columns], preferred_element_type=f32
        )
        return carry

    lax.fori_loop(0, width // span, shared_step, 0)

    for dz, r in peers:
        route_copy(dz, r, True).wait_recv()
    for a in range(3):
        landed(trio(1)[a], s["wtr"].at[a])

    def forward(p):
        t = level_at(z, p)
        for c in range(pieces):
            landed(tok.at[t, 0, part(c)], s["zr"].at[t, c])
            spread(tok.at[t, 0, part(c)], t, c)

    def relay(a):
        for k in range(a * WEIGHT_CUTS, (a + 1) * WEIGHT_CUTS):
            target = trio(2)[a]
            size = target.shape[0] // WEIGHT_CUTS
            landed(target.at[pl.ds(k % WEIGHT_CUTS * size, size)], s["wxr"].at[k])
        core_copy(2, a).start()

    expert_lane = lax.broadcasted_iota(jnp.int32, (count, LANES), 1)

    def scale_column(slot, expert):
        table = jnp.concatenate(
            [s["route"][slot], jnp.zeros((LANES - experts, count), f32)], axis=0
        )
        picked = jnp.where(expert_lane == expert, jnp.transpose(table), 0.0)
        return jnp.sum(picked, axis=1, keepdims=True)

    def give(t):
        for c in range(pieces):
            y_copy(t, c).start()

    def y_copy(t, c):
        return remote(
            y_out.at[t, part(c)], y_in.at[t, part(c)], s["rys"].at[t, c], s["ryr"].at[t, c],
            beside,
        )

    hidden = s["hidden"]

    def step(i, carry):
        p = jnp.where(i < 6, lax.rem(i, 3), 3)
        e = jnp.where(i < 6, i // 3, i - 6)
        t = level_at(z, p)

        @pl.when(i == 0)
        def _():
            forward(1)
            forward(2)

        @pl.when(i == 1)
        def _():
            forward(3)
            relay(0)

        @pl.when(i == 2)
        def _():
            relay(1)

        @pl.when(i == 3)
        def _():
            relay(2)
            for a in range(3):
                landed(trio(3)[a], s["wtr"].at[3 + a])

        @pl.when(e == 0)
        def _():
            for c in range(pieces):
                landed(tok.at[t, 1, part(c)], s["yr"].at[t, c])

        expert = jnp.where(e == 0, me, pair)
        scale = jnp.concatenate(
            [scale_column(t * 2, expert), scale_column(t * 2 + 1, expert)], axis=0
        )

        def inner(j, carry):
            block = tok[t].reshape(2 * count, width)
            gate = jnp.dot(block, wg[2 * e + j], preferred_element_type=f32)
            upward = jnp.dot(block, wu[2 * e + j], preferred_element_type=f32)
            columns = pl.ds(pl.multiple_of(j * half, half), half)
            hidden[:, columns] = (jax.nn.silu(gate) * upward * scale).astype(bf16)
            return carry

        lax.fori_loop(0, 2, inner, 0)

        def outer(k, carry):
            columns = pl.ds(pl.multiple_of(k * span, span), span)
            depth = pl.ds(pl.multiple_of(e * 2 * half, 2 * half), 2 * half)
            result = jnp.dot(hidden[...], wd[depth, columns], preferred_element_type=f32)

            @pl.when(e == 0)
            def _():
                acc[t, :, columns] = result

            @pl.when(e == 1)
            def _():
                whole = acc[t, :, columns] + result
                acc[t, :, columns] = whole
                y_out[t, :, columns] = whole[count:].astype(bf16)

            return carry

        lax.fori_loop(0, width // span, outer, 0)

        @pl.when(i == 5)
        def _():
            give(level_at(z, 2))

        @pl.when(i == 7)
        def _():
            give(level_at(z, 3))
            give(level_at(z, 1))
            give(level_at(z, 0))

        return carry

    lax.fori_loop(0, 8, step, 0)

    def take(t, c):
        landed(y_in.at[t, part(c)], s["ryr"].at[t, c])

    def arrive(slot, c):
        landed(z_in.at[slot, part(c)], s["rzr"].at[slot, c])

    def hop(p, c):
        t = level_at(z, p)
        up = t > z
        slot = jnp.where(up | (t < z - 1), t, LEVELS)
        return remote(
            z_out.at[t, part(c)],
            z_in.at[slot, part(c)],
            s["rzs"].at[t, c],
            s["rzr"].at[slot, c],
            jnp.where(up, above, below),
        )

    for p in (2, 3, 1):
        t = level_at(z, p)
        up = t > z
        fed = (up & (z > 0)) | (jnp.logical_not(up) & (z < LEVELS - 1))
        for c in range(pieces):
            take(t, c)

            @pl.when(fed)
            def _():
                arrive(t, c)
                z_out[t, part(c)] = (
                    acc[t, part(c)]
                    + y_in[t, part(c)].astype(f32)
                    + z_in[t, part(c)].astype(f32)
                ).astype(bf16)

            @pl.when(jnp.logical_not(fed))
            def _():
                z_out[t, part(c)] = (
                    acc[t, part(c)] + y_in[t, part(c)].astype(f32)
                ).astype(bf16)

            hop(p, c).start()

    for c in range(pieces):
        shared_out[part(c)] += acc[z, part(c)]

        @pl.when(z > 0)
        def _():
            arrive(z, c)
            shared_out[part(c)] += z_in[z, part(c)].astype(f32)

        @pl.when(z < LEVELS - 1)
        def _():
            arrive(LEVELS, c)
            shared_out[part(c)] += z_in[LEVELS, part(c)].astype(f32)

        take(z, c)
        out_ref[part(c)] = (
            shared_out[part(c)] + y_in[z, part(c)].astype(f32)
        ).astype(out_ref.dtype)

    for copy in swaps:
        copy.wait_send()

    @pl.when(x == 0)
    def _():
        query_send(1)[0].wait_send()

    @pl.when(x == 1)
    def _():
        query_send(0)[1].wait_send()
        query_send(1)[1].wait_send()
        attended_copy(0, 0).wait_send()

    attended_copy(1, 0).wait_send()
    attended_copy(1, 1).wait_send()
    attended_copy(0, 1).wait_send()
    for k in range(3 * WEIGHT_CUTS):
        weight_piece(k).wait_send()
    for a in range(3):
        core_copy(0, a).wait_send()
        core_copy(2, a).wait_send()
    for dz, r in peers:
        route_copy(dz, r, False).wait_send()

    def drain(t, carry):
        for k in range(2):
            b = chip(t, y, k)

            @pl.when((t <= z) & (z < LEVELS - 1))
            def _():
                kv_along(b, True).wait_send()

            @pl.when((t >= z) & (z > 0))
            def _():
                kv_along(b, False).wait_send()

            kv_across(b).wait_send()
        for c in range(pieces):
            @pl.when((t <= z) & (z < LEVELS - 1))
            def _():
                along(tok.at[t, 0, part(c)], t, c, True).wait_send()

            @pl.when((t >= z) & (z > 0))
            def _():
                along(tok.at[t, 0, part(c)], t, c, False).wait_send()

            across(tok.at[t, 0, part(c)], t, c).wait_send()
            y_copy(t, c).wait_send()
        return carry

    lax.fori_loop(0, LEVELS, drain, 0)
    for p in (1, 2, 3):
        for c in range(pieces):
            hop(p, c).wait_send()


def whole_layer(blocks, vmem_arrays, hbm_arrays, number):
    count, width = vmem_arrays["residual"].shape
    tokens = vmem_arrays["query"].shape[0]
    half = hbm_arrays["gate"].shape[1]
    middle = hbm_arrays["shared_gate"].shape[1]
    heads_width = hbm_arrays["project"].shape[0]
    pieces = 4
    vmem, hbm = pl.BlockSpec(memory_space=pltpu.VMEM), pl.BlockSpec(memory_space=pl.ANY)
    bf16, f32 = jnp.bfloat16, jnp.float32
    dma = pltpu.SemaphoreType.DMA
    scratch = {
        "kv": pltpu.VMEM((blocks, 2, tokens, LANES), bf16),
        "qs": pltpu.VMEM((2, tokens, LANES), bf16),
        "qm": pltpu.VMEM((2, 2, tokens, LANES), bf16),
        "after": pltpu.VMEM((tokens, tokens), bf16),
        "seg": pltpu.VMEM((2, LEVELS, tokens, LANES), f32),
        "sum": pltpu.VMEM((2, LEVELS, tokens, LANES), f32),
        "ob": pltpu.VMEM((2, tokens, LANES), bf16),
        "att": pltpu.VMEM((heads_width // LANES, count, LANES), bf16),
        "wo": pltpu.VMEM((heads_width, width), bf16),
        "mixed": pltpu.VMEM((count, width), bf16),
        "normed": pltpu.VMEM((count, width), bf16),
        "tok": pltpu.VMEM((LEVELS, 2, count, width), bf16),
        "acc": pltpu.VMEM((LEVELS, 2 * count, width), f32),
        "wg": pltpu.VMEM((4, width, half), bf16),
        "wu": pltpu.VMEM((4, width, half), bf16),
        "wd": pltpu.VMEM((4 * half, width), bf16),
        "sg": pltpu.VMEM((width, middle), bf16),
        "su": pltpu.VMEM((width, middle), bf16),
        "sd": pltpu.VMEM((middle, width), bf16),
        "shared_out": pltpu.VMEM((count, width), f32),
        "hidden": pltpu.VMEM((2 * count, 2 * half), bf16),
        "shared_hidden": pltpu.VMEM((count, middle), bf16),
        "y_out": pltpu.VMEM((LEVELS, count, width), bf16),
        "y_in": pltpu.VMEM((LEVELS, count, width), bf16),
        "z_out": pltpu.VMEM((LEVELS, count, width), bf16),
        "z_in": pltpu.VMEM((LEVELS + 1, count, width), bf16),
        "route": pltpu.VMEM((2 * LEVELS,) + vmem_arrays["table"].shape, f32),
        "idle": dma((1,)),
        "load_sem": dma((len(hbm_arrays),)),
        "near_sem": dma((3,)),
        "kxs": dma((2,)),
        "kxr": dma((2,)),
        "qss": dma((2,)),
        "qsr": dma((2,)),
        "kzs": dma((2, blocks)),
        "kzr": dma((blocks,)),
        "kys": dma((blocks,)),
        "kyr": dma((blocks,)),
        "oss": dma((2, 2)),
        "osr": dma((4,)),
        "wts": dma((6,)),
        "wtr": dma((6,)),
        "wxs": dma((3 * WEIGHT_CUTS,)),
        "wxr": dma((3 * WEIGHT_CUTS,)),
        "w_send": dma((LEVELS, 2)),
        "w_recv": dma((LEVELS, 2)),
        "zs": dma((2, LEVELS, pieces)),
        "zr": dma((LEVELS, pieces)),
        "ys": dma((LEVELS, pieces)),
        "yr": dma((LEVELS, pieces)),
        "rys": dma((LEVELS, pieces)),
        "ryr": dma((LEVELS, pieces)),
        "rzs": dma((LEVELS, pieces)),
        "rzr": dma((LEVELS + 1, pieces)),
    }
    names = list(vmem_arrays) + list(hbm_arrays) + ["out"] + list(scratch)
    return pl.pallas_call(
        functools.partial(layer_kernel, pieces, names),
        out_shape=jax.ShapeDtypeStruct((count, width), bf16),
        in_specs=[vmem] * len(vmem_arrays) + [hbm] * len(hbm_arrays),
        out_specs=vmem,
        scratch_shapes=list(scratch.values()),
        compiler_params=pltpu.CompilerParams(
            collective_id=number,
            has_side_effects=True,
            vmem_limit_bytes=60 * 1024 * 1024,
        ),
    )(*vmem_arrays.values(), *hbm_arrays.values())


def expert_product(rows, gate_half, up_half, down_half):
    gate = jnp.einsum("seid,edf->seif", rows, gate_half, preferred_element_type=jnp.float32)
    upward = jnp.einsum("seid,edf->seif", rows, up_half, preferred_element_type=jnp.float32)
    hidden = (jax.nn.silu(gate) * upward).astype(jnp.bfloat16)
    return jnp.einsum("seif,efd->seid", hidden, down_half, preferred_element_type=jnp.float32)


def local(
    queries,
    key_rows,
    value_rows,
    residual,
    out_weight,
    norm_gain,
    routes,
    route_weight,
    expert_gate,
    expert_up,
    expert_down,
    shared_gate,
    shared_up,
    shared_down,
):
    query_count = queries.shape[0]
    local_width = queries.shape[1]
    blocks = lax.axis_size("sp")
    experts_all = blocks * expert_gate.shape[0]
    if (
        blocks == 4 * LEVELS
        and expert_gate.shape[0] == 1
        and lax.axis_size("tp") == 2
        and local_width == 2 * LANES
    ):
        picked = routes[:, :, None] == jnp.arange(experts_all, dtype=jnp.int32)
        table = jnp.sum(jnp.where(picked, route_weight[:, :, None], 0.0), axis=1)
        return whole_layer(
            blocks,
            {
                "query": queries,
                "key": key_rows,
                "value": value_rows,
                "residual": residual,
                "gain": norm_gain[None, :],
                "table": table.T,
            },
            {
                "gate": expert_gate[0],
                "up": expert_up[0],
                "down": expert_down[0],
                "project": out_weight,
                "shared_gate": shared_gate,
                "shared_up": shared_up,
                "shared_down": shared_down,
            },
            3,
        )
    kv = jnp.concatenate([key_rows, value_rows], axis=1)
    kv = gather(kv, blocks, 0).reshape(-1, kv.shape[1])
    attended = attention(queries, kv)
    token_rows = residual.shape[0]
    weight_rows = lax.dynamic_slice_in_dim(
        out_weight, lax.axis_index("tp") * local_width, local_width, 0
    )
    projected = lax.psum_scatter(
        jnp.dot(attended, weight_rows, preferred_element_type=jnp.float32),
        "tp",
        scatter_dimension=0,
        tiled=True,
    )
    mixed_wide = (residual.astype(jnp.float32) + projected).astype(jnp.bfloat16).astype(jnp.float32)
    inverse = lax.rsqrt(jnp.mean(mixed_wide * mixed_wide, axis=1, keepdims=True) + norm_eps)
    normed = (mixed_wide * inverse * norm_gain).astype(jnp.bfloat16)
    width = normed.shape[1]
    local_experts = expert_gate.shape[0]
    experts_all = blocks * local_experts
    capacity = max(2, token_rows * TOPK * 5 // (4 * experts_all))
    flat_routes = routes.reshape(-1)
    picks = (flat_routes[:, None] == jnp.arange(experts_all, dtype=jnp.int32)[None, :]).astype(
        jnp.int32
    )
    earlier = jnp.cumsum(picks, axis=0) - picks
    position = flat_routes * capacity + jnp.sum(earlier * picks, axis=1)
    filler = (
        jnp.zeros((experts_all * capacity,), jnp.int32)
        .at[position]
        .set(jnp.arange(flat_routes.shape[0], dtype=jnp.int32) + 1)
    )
    occupied = filler > 0
    source_token = jnp.maximum(filler - 1, 0) // TOPK
    outgoing = jnp.where(
        occupied[:, None], normed[source_token], jnp.zeros((), jnp.bfloat16)
    ).reshape(experts_all, capacity, width)
    both = lax.all_gather(
        exchange(
            outgoing.reshape(blocks, local_experts * capacity, width), blocks, 1
        ).reshape(outgoing.shape),
        "tp",
        axis=0,
        tiled=True,
    )
    shaped = both.reshape(-1, local_experts, both.shape[1], both.shape[2])
    pieces = expert_product(shaped, expert_gate, expert_up, expert_down).reshape(both.shape)
    summed = lax.psum_scatter(pieces.astype(jnp.bfloat16), "tp", scatter_dimension=0, tiled=True)
    results = exchange(
        summed.reshape(blocks, local_experts * capacity, width), blocks, 2
    ).reshape(
        experts_all * capacity, width
    )
    picked = results[position].reshape(token_rows, TOPK, width)
    routed = jnp.sum(picked.astype(jnp.float32) * route_weight[:, :, None], axis=1)
    shared_gate_out = jnp.dot(normed, shared_gate, preferred_element_type=jnp.float32)
    shared_up_out = jnp.dot(normed, shared_up, preferred_element_type=jnp.float32)
    shared_act = (jax.nn.silu(shared_gate_out) * shared_up_out).astype(jnp.bfloat16)
    shared_out = jnp.dot(shared_act, shared_down, preferred_element_type=jnp.float32)
    return (mixed_wide + routed + shared_out).astype(jnp.bfloat16)


def solution(mesh):
    return jax.shard_map(
        local,
        mesh=mesh,
        in_specs=(
            P("sp", "tp"),
            P("sp", "tp"),
            P("sp", "tp"),
            P(("sp", "tp"), None),
            P(),
            P(),
            P(("sp", "tp"), None),
            P(("sp", "tp"), None),
            P("sp", None, "tp"),
            P("sp", None, "tp"),
            P("sp", "tp", None),
            P(),
            P(),
            P(),
        ),
        out_specs=P(("sp", "tp"), None),
        check_vma=False,
    )
```

```python
import functools

import jax
import jax.numpy as jnp
from jax import lax
from jax.experimental import pallas as pl
from jax.experimental.pallas import tpu as pltpu
from jax.sharding import PartitionSpec as P

HEAD_DIM = 64
TOPK = 8


norm_eps = 1e-06


MESH = pl.DeviceIdType.MESH
LANES = 128


def attention_kernel(query_ref, kv_ref, out_ref, acc_ref, later_ref):
    own = lax.axis_index("sp")
    count, width = query_ref.shape
    lane = lax.broadcasted_iota(jnp.int32, (count, LANES), 1)
    row = lax.broadcasted_iota(jnp.int32, (count, count), 0)
    column = lax.broadcasted_iota(jnp.int32, (count, count), 1)
    after = (row > column).astype(jnp.bfloat16)
    acc_ref[...] = jnp.zeros_like(acc_ref)
    later_ref[...] = jnp.zeros_like(later_ref)

    def tile(block, diagonal):
        rows = pl.ds(pl.multiple_of(block * count, count), count)
        for pair in range(width // LANES):
            columns = slice(pair * LANES, (pair + 1) * LANES)
            keys = kv_ref[rows, columns]
            values = kv_ref[rows, width + pair * LANES : width + (pair + 1) * LANES]
            sides = []
            for side in range(LANES // HEAD_DIM):
                head = pair * (LANES // HEAD_DIM) + side
                mine = (lane >= side * HEAD_DIM) & (lane < (side + 1) * HEAD_DIM)
                query = query_ref[:, columns].astype(jnp.float32) * HEAD_DIM ** (-0.5)
                query = jnp.where(mine, query, 0.0).astype(jnp.bfloat16)
                scores = lax.dot_general(
                    query, keys, (((1,), (1,)), ((), ())), preferred_element_type=jnp.float32
                )
                tail = jnp.log(1.0 + jnp.exp(-jnp.abs(scores)))
                cost = jnp.maximum(scores, 0.0) + tail
                if diagonal:
                    cost = jnp.where(column < row, cost, 0.0)
                high = cost.astype(jnp.bfloat16)
                low = (cost - high.astype(jnp.float32)).astype(jnp.bfloat16)
                inside = jnp.dot(high, after, preferred_element_type=jnp.float32)
                inside = inside + jnp.dot(low, after, preferred_element_type=jnp.float32)
                weight = jnp.exp(jnp.minimum(scores, 0.0) - tail - inside)
                if diagonal:
                    weight = jnp.where(column < row, weight, 0.0)
                partial = jnp.dot(
                    weight.astype(jnp.bfloat16), values, preferred_element_type=jnp.float32
                )
                later = later_ref[head]
                sides.append(jnp.exp(-later) * partial)
                total = inside[:, 0:1] + cost[:, 0:1]
                later_ref[head] = later + jnp.broadcast_to(total, later.shape)
            acc_ref[:, columns] += jnp.where(lane < HEAD_DIM, sides[0], sides[1])

    tile(own, True)

    def step(index, carry):
        tile(own - 1 - index, False)
        return carry

    lax.fori_loop(0, own, step, 0)
    out_ref[...] = acc_ref[...].astype(out_ref.dtype)


def attention(queries, kv):
    count, width = queries.shape
    return pl.pallas_call(
        attention_kernel,
        out_shape=jax.ShapeDtypeStruct((count, width), jnp.bfloat16),
        in_specs=[pl.BlockSpec(memory_space=pltpu.VMEM)] * 2,
        out_specs=pl.BlockSpec(memory_space=pltpu.VMEM),
        scratch_shapes=[
            pltpu.VMEM((count, width), jnp.float32),
            pltpu.VMEM((width // HEAD_DIM, count, LANES), jnp.float32),
        ],
        compiler_params=pltpu.CompilerParams(vmem_limit_bytes=56 * 1024 * 1024),
    )(queries, kv)


def gather_kernel(n, depth, in_ref, out_ref, stage, send_sem, recv_sem, local_sem):
    me = lax.axis_index("sp")
    plane = n // depth
    level, place = me // plane, lax.rem(me, plane)

    def above(k):
        return lax.rem(level + k, depth) * plane + place

    def beside(j):
        return level * plane + lax.rem(place + j, plane)

    peers = [above(k) for k in range(1, depth)] + [beside(j) for j in range(1, plane)]
    barrier = pltpu.get_barrier_semaphore()
    for peer in peers:
        pl.semaphore_signal(barrier, inc=1, device_id={"sp": peer}, device_id_type=MESH)
    pl.semaphore_wait(barrier, len(peers))

    def send(source, block, peer, k, j):
        copy = pltpu.make_async_remote_copy(
            src_ref=source,
            dst_ref=out_ref.at[block],
            send_sem=send_sem.at[k, j],
            recv_sem=recv_sem.at[k, j],
            device_id={"sp": peer},
            device_id_type=MESH,
        )
        copy.start()
        return copy

    rising = [send(in_ref, me, above(k), k, 0) for k in range(1, depth)]
    level_copies = [send(in_ref, me, beside(j), 0, j) for j in range(1, plane)]
    inward = pltpu.make_async_copy(in_ref, stage, local_sem)
    inward.start()
    inward.wait()
    outward = pltpu.make_async_copy(stage, out_ref.at[me], local_sem)
    outward.start()
    outward.wait()
    for k in range(1, depth):
        rising[k - 1].wait_recv()
        block = lax.rem(level + depth - k, depth) * plane + place
        for j in range(1, plane):
            level_copies.append(send(out_ref.at[block], block, beside(j), k, j))
    for copy in rising:
        copy.wait_send()
    for copy in level_copies:
        copy.wait()


def gather(array, n, number):
    depth = 4 if n % 4 == 0 else 1
    return pl.pallas_call(
        functools.partial(gather_kernel, n, depth),
        out_shape=jax.ShapeDtypeStruct((n,) + array.shape, array.dtype),
        in_specs=[pl.BlockSpec(memory_space=pltpu.HBM)],
        out_specs=pl.BlockSpec(memory_space=pltpu.HBM),
        scratch_shapes=[
            pltpu.VMEM(array.shape, array.dtype),
            pltpu.SemaphoreType.DMA((depth, n // depth)),
            pltpu.SemaphoreType.DMA((depth, n // depth)),
            pltpu.SemaphoreType.DMA,
        ],
        compiler_params=pltpu.CompilerParams(collective_id=number, has_side_effects=True),
    )(array)


def exchange_kernel(n, in_ref, out_ref, stage, send_sem, recv_sem, local_sem):
    me = lax.axis_index("sp")
    barrier = pltpu.get_barrier_semaphore()
    for k in range(1, n):
        pl.semaphore_signal(
            barrier, inc=1, device_id={"sp": lax.rem(me + k, n)}, device_id_type=MESH
        )
    pl.semaphore_wait(barrier, n - 1)

    def part(peer):
        return in_ref.at[peer]

    copies = []
    for k in range(1, n):
        peer = lax.rem(me + k, n)
        copy = pltpu.make_async_remote_copy(
            src_ref=part(peer),
            dst_ref=out_ref.at[me],
            send_sem=send_sem.at[k],
            recv_sem=recv_sem.at[k],
            device_id={"sp": peer},
            device_id_type=MESH,
        )
        copy.start()
        copies.append(copy)
    inward = pltpu.make_async_copy(part(me), stage, local_sem)
    inward.start()
    inward.wait()
    outward = pltpu.make_async_copy(stage, out_ref.at[me], local_sem)
    outward.start()
    outward.wait()
    for copy in copies:
        copy.wait()


def exchange(array, n, number):
    shape = array.shape[1:]
    return pl.pallas_call(
        functools.partial(exchange_kernel, n),
        out_shape=jax.ShapeDtypeStruct((n,) + shape, array.dtype),
        in_specs=[pl.BlockSpec(memory_space=pltpu.HBM)],
        out_specs=pl.BlockSpec(memory_space=pltpu.HBM),
        scratch_shapes=[
            pltpu.VMEM(shape, array.dtype),
            pltpu.SemaphoreType.DMA((n,)),
            pltpu.SemaphoreType.DMA((n,)),
            pltpu.SemaphoreType.DMA,
        ],
        compiler_params=pltpu.CompilerParams(collective_id=number, has_side_effects=True),
    )(array)


LEVELS = 4
FIRST_SHIPPED = 4
SHIPPED = 11
SHIP_RATE = 2
WEIGHT_CUTS = 8


def level_at(z, p):
    low = z * 2 < LEVELS
    place = jnp.where(low, z, LEVELS - 1 - z)
    step = jnp.where(p == 0, place, jnp.where(p - 1 < place, p - 1, p))
    return jnp.where(low, step, LEVELS - 1 - step)


def layer_kernel(pieces, names, *refs):
    s = dict(zip(names, refs))
    f32, bf16 = jnp.float32, jnp.bfloat16
    me, core = lax.axis_index("sp"), lax.axis_index("tp")
    x, y, z = lax.rem(me, 2), lax.rem(me // 2, 2), me // 4
    out_ref = s["out"]
    count, width = out_ref.shape
    tokens = s["query"].shape[0]
    blocks = s["kv"].shape[0]
    experts = s["table"].shape[0]
    half = s["wg"].shape[2]
    rows = count // pieces
    span = min(width, 512)

    def chip(level, side, place):
        return level * 4 + side * 2 + place

    def remote(source, target, send, recv, peer, peer_core=None):
        return pltpu.make_async_remote_copy(
            src_ref=source,
            dst_ref=target,
            send_sem=send,
            recv_sem=recv,
            device_id={"sp": peer, "tp": core if peer_core is None else peer_core},
            device_id_type=MESH,
        )

    pair = me + 1 - 2 * x
    beside = chip(z, 1 - y, x)
    above, below = me + 4, me - 4
    mirror = chip(LEVELS - 1 - z, 1 - y, 0)

    def landed(target, recv):
        remote(target, target, s["idle"].at[0], recv, beside).wait_recv()

    wg, wu, wd = s["wg"], s["wu"], s["wd"]

    def trio(j):
        return wg.at[j], wu.at[j], wd.at[pl.ds(j * half, half)]

    loads = list(zip((s["gate"], s["up"], s["down"]), trio(0)))
    loads += [(s["project"], s["wo"])]
    loads += list(zip((s["shared_gate"], s["shared_up"], s["shared_down"]), (s["sg"], s["su"], s["sd"])))
    loads = [
        pltpu.make_async_copy(source, target, s["load_sem"].at[k])
        for k, (source, target) in enumerate(loads)
    ]
    for load in loads:
        load.start()

    def lanes(place):
        return pl.ds(pl.multiple_of(place * LANES, LANES), LANES)

    kv = s["kv"]
    near = [
        pltpu.make_async_copy(s[name].at[:, lanes(x)], kv.at[me, k], s["near_sem"].at[k])
        for k, name in enumerate(("key", "value"))
    ]
    for copy in near:
        copy.start()

    barrier = pltpu.get_barrier_semaphore()
    peers = [(dz, r) for dz in range(LEVELS) for r in range(2) if (dz, r) != (0, 0)]
    greeted = [
        (chip(lax.rem(z + dz, LEVELS), lax.rem(y + r, 2), x), core) for dz, r in peers
    ]
    greeted += [(me, 1 - core), (pair, core), (pair, 1 - core)]
    greeted += [(mirror + x, 1 - core), (mirror + 1 - x, core), (mirror + 1 - x, 1 - core)]
    for peer, peer_core in greeted:
        pl.semaphore_signal(
            barrier, inc=1, device_id={"sp": peer, "tp": peer_core}, device_id_type=MESH
        )
    pl.semaphore_wait(barrier, len(greeted))

    swaps = [
        remote(
            s[name].at[:, lanes(1 - x)], kv.at[me, k], s["kxs"].at[k], s["kxr"].at[k], pair
        )
        for k, name in enumerate(("key", "value"))
    ]
    for copy in swaps:
        copy.start()

    query, qs = s["query"], s["qs"]
    kept = pltpu.make_async_copy(query.at[:, lanes(0)], qs.at[0], s["near_sem"].at[2])

    def query_keep():
        return remote(
            query.at[:, lanes(1)], qs.at[0], s["qss"].at[1], s["qsr"].at[0], pair
        )

    def query_move(place):
        return remote(
            query.at[:, lanes(place)], qs.at[1], s["qss"].at[place], s["qsr"].at[1],
            mirror + place,
        )

    @pl.when(x == 0)
    def _():
        kept.start()
        query_keep().start()

    @pl.when(x == 1)
    def _():
        query_move(0).start()
        query_move(1).start()

    def weight_piece(k):
        a, r = k // WEIGHT_CUTS, k % WEIGHT_CUTS
        source, target = (s["gate"], s["up"], s["down"])[a], trio(2)[a]
        size = source.shape[0] // WEIGHT_CUTS
        cut = pl.ds(r * size, size)
        return remote(source.at[cut], target.at[cut], s["wxs"].at[k], s["wxr"].at[k], pair)

    for k in range(FIRST_SHIPPED):
        weight_piece(k).start()

    def kv_along(b, up):
        return remote(
            kv.at[b], kv.at[b], s["kzs"].at[0 if up else 1, b], s["kzr"].at[b],
            above if up else below,
        )

    def kv_across(b):
        return remote(kv.at[b], kv.at[b], s["kys"].at[b], s["kyr"].at[b], beside)

    def kv_spread(b):
        t = b // 4

        @pl.when((t <= z) & (z < LEVELS - 1))
        def _():
            kv_along(b, True).start()

        @pl.when((t >= z) & (z > 0))
        def _():
            kv_along(b, False).start()

        kv_across(b).start()

    for copy in near:
        copy.wait()
    kv_spread(me)

    def route_copy(dz, r, incoming):
        origin = lax.rem(z + LEVELS - dz, LEVELS) if incoming else z
        peer = chip(lax.rem(z + dz, LEVELS), lax.rem(y + r, 2), x)
        return remote(
            s["table"], s["route"].at[origin * 2 + r], s["w_send"].at[dz, r],
            s["w_recv"].at[dz, r], peer,
        )

    for dz, r in peers:
        route_copy(dz, r, False).start()
    s["route"][z * 2] = s["table"][...]

    def core_copy(j, a):
        k = 3 * (j // 2) + a
        return remote(
            trio(j)[a], trio(j + 1)[a], s["wts"].at[k], s["wtr"].at[k], me, 1 - core
        )

    row = lax.broadcasted_iota(jnp.int32, (tokens, tokens), 0)
    column = lax.broadcasted_iota(jnp.int32, (tokens, tokens), 1)
    s["after"][...] = (row > column).astype(bf16)
    s["seg"][...] = jnp.zeros_like(s["seg"])
    s["sum"][...] = jnp.zeros_like(s["sum"])

    for k in range(2):
        landed(kv.at[pair, k], s["kxr"].at[k])
    kv_spread(pair)

    def kv_forward(p, mine):
        b = chip(level_at(z, p), y, x if mine else 1 - x)
        landed(kv.at[b], s["kzr"].at[b])
        kv_spread(b)

    edge = (z == 0) | (z == LEVELS - 1)
    inner_level = jnp.logical_not(edge)
    kv_forward(1, True)

    @pl.when(inner_level)
    def _():
        kv_forward(2, True)

    for load in loads[:3]:
        load.wait()
    for a in range(3):
        core_copy(0, a).start()
    @pl.when(x == 0)
    def _():
        kept.wait()

    @pl.when(x == 1)
    def _():
        landed(qs.at[0], s["qsr"].at[0])

    landed(qs.at[1], s["qsr"].at[1])
    lane = lax.broadcasted_iota(jnp.int32, (tokens, LANES), 1)
    first = lane < HEAD_DIM
    for f in range(2):
        scaled = qs[f].astype(f32) * HEAD_DIM ** (-0.5)
        s["qm"][f, 0] = jnp.where(first, scaled, 0.0).astype(bf16)
        s["qm"][f, 1] = jnp.where(first, 0.0, scaled).astype(bf16)

    def tile(f, t, b, diagonal):
        parts, totals = [], []
        for h in range(2):
            scores = lax.dot_general(
                s["qm"][f, h], kv[b, 0], (((1,), (1,)), ((), ())), preferred_element_type=f32
            )
            tail = jnp.log(1.0 + jnp.exp(-jnp.abs(scores)))
            cost = jnp.maximum(scores, 0.0) + tail
            if diagonal:
                mask = lax.broadcasted_iota(
                    jnp.int32, (tokens, tokens), 1
                ) < lax.broadcasted_iota(jnp.int32, (tokens, tokens), 0)
                cost = jnp.where(mask, cost, 0.0)
            high = cost.astype(bf16)
            low = (cost - high.astype(f32)).astype(bf16)
            inside = jnp.dot(high, s["after"][...], preferred_element_type=f32)
            inside = inside + jnp.dot(low, s["after"][...], preferred_element_type=f32)
            weight = jnp.exp(jnp.minimum(scores, 0.0) - tail - inside)
            if diagonal:
                weight = jnp.where(mask, weight, 0.0)
            parts.append(jnp.dot(weight.astype(bf16), kv[b, 1], preferred_element_type=f32))
            totals.append(inside[:, 0:1] + cost[:, 0:1])
        total = jnp.where(first, totals[0], totals[1])
        s["seg"][f, t] = s["seg"][f, t] * jnp.exp(-total) + jnp.where(first, parts[0], parts[1])
        s["sum"][f, t] += total

    kept_block = chip(z, y, 0)
    order = ((0, 0), (0, 1), (1, 0), (2, 0), (1, 1), (3, 0), (2, 1), (3, 1))

    def attend(i, carry):
        p = functools.reduce(lambda a, k: jnp.where(i == k, order[k][0], a), range(1, 8), 0)
        far = functools.reduce(lambda a, k: jnp.where(i == k, order[k][1], a), range(1, 8), 0)

        @pl.when(i == 1)
        def _():
            kv_forward(1, False)

        for at, far_level, mine in ((1, 2, True), (2, 2, False), (3, 3, True), (4, 3, False)):
            @pl.when((i == at) & edge)
            def _():
                kv_forward(far_level, mine)

        for at, far_level, mine in ((1, 2, False), (2, 3, True), (3, 3, False)):
            @pl.when((i == at) & inner_level)
            def _():
                kv_forward(far_level, mine)

        t = level_at(z, p)
        side = jnp.where(far == 1, 1 - y, y)
        start = chip(t, side, 0)
        segment = start // 2

        @pl.when(far == 1)
        def _():
            for k in range(2):
                landed(kv.at[start + k], s["kyr"].at[start + k])

        def one_query(f, carry):
            block = jnp.where(f == 0, kept_block, blocks - 1 - kept_block)
            full = jnp.clip(block - start, 0, 2)

            def one_key(b, carry):
                tile(f, segment, start + b, False)
                return carry

            lax.fori_loop(0, full, one_key, 0)

            @pl.when((block >= start) & (block < start + 2))
            def _():
                tile(f, segment, block, True)

            return carry

        lax.fori_loop(0, 2, one_query, 0)

        for k in range(FIRST_SHIPPED, SHIPPED):
            @pl.when(i == (k - FIRST_SHIPPED) // SHIP_RATE)
            def _():
                weight_piece(k).start()

        return carry

    lax.fori_loop(0, 2 * LEVELS, attend, 0)

    for f in range(2):
        later = s["sum"][f, 2 * LEVELS - 1]
        value = s["seg"][f, 2 * LEVELS - 1]
        for t in reversed(range(2 * LEVELS - 1)):
            value = value + jnp.exp(-later) * s["seg"][f, t]
            later = later + s["sum"][f, t]
        s["ob"][f] = value.astype(bf16)

    spot = core * 2 + x

    def attended_copy(f, d):
        other = lax.rem(core + d, 2)
        source = s["ob"].at[f, pl.ds(pl.multiple_of(other * count, count), count)]
        target = kept_block if f == 0 else mirror + 1
        return remote(
            source, s["att"].at[spot], s["oss"].at[f, d], s["osr"].at[spot], target, other
        )

    attended_copy(1, 0).start()
    attended_copy(1, 1).start()
    attended_copy(0, 1).start()

    @pl.when(x == 1)
    def _():
        attended_copy(0, 0).start()

    @pl.when(x == 0)
    def _():
        s["att"][spot] = s["ob"][0, pl.ds(pl.multiple_of(core * count, count), count)]

    loads[3].wait()
    for k in range(4):
        @pl.when((x == 1) | (k != spot))
        def _():
            landed(s["att"].at[k], s["osr"].at[k])

    for k in range(SHIPPED, 3 * WEIGHT_CUTS):
        weight_piece(k).start()

    mixed, normed = s["mixed"], s["normed"]
    attended = jnp.concatenate([s["att"][k] for k in range(4)], axis=1)

    def project_step(k, carry):
        columns = pl.ds(pl.multiple_of(k * span, span), span)
        value = s["residual"][:, columns].astype(f32) + jnp.dot(
            attended, s["wo"][:, columns], preferred_element_type=f32
        )
        value = value.astype(bf16)
        mixed[:, columns] = value
        value = value.astype(f32)
        return carry + jnp.sum(value * value, axis=1, keepdims=True)

    squares = lax.fori_loop(0, width // span, project_step, jnp.zeros((count, 1), f32))
    inverse = lax.rsqrt(squares / width + norm_eps)
    for k in range(width // span):
        columns = slice(k * span, (k + 1) * span)
        normed[:, columns] = (
            mixed[:, columns].astype(f32) * inverse * s["gain"][:, columns]
        ).astype(bf16)

    tok, acc = s["tok"], s["acc"]
    y_out, y_in, z_out, z_in = s["y_out"], s["y_in"], s["z_out"], s["z_in"]

    def part(c):
        return pl.ds(c * rows, rows)

    def along(source, t, c, up):
        return remote(
            source,
            tok.at[t, 0, part(c)],
            s["zs"].at[0 if up else 1, t, c],
            s["zr"].at[t, c],
            above if up else below,
        )

    def across(source, t, c):
        return remote(
            source, tok.at[t, 1, part(c)], s["ys"].at[t, c], s["yr"].at[t, c], beside
        )

    def spread(source, t, c):
        @pl.when((t <= z) & (z < LEVELS - 1))
        def _():
            along(source, t, c, True).start()

        @pl.when((t >= z) & (z > 0))
        def _():
            along(source, t, c, False).start()

        across(source, t, c).start()

    tok[z, 0] = normed[...]
    for c in range(pieces):
        spread(normed.at[part(c)], z, c)

    for load in loads[4:]:
        load.wait()
    shared_out = s["shared_out"]
    shared_half = s["sg"].shape[1] // 2
    for j in range(2):
        columns = slice(j * shared_half, (j + 1) * shared_half)
        gate = jnp.dot(normed[...], s["sg"][:, columns], preferred_element_type=f32)
        upward = jnp.dot(normed[...], s["su"][:, columns], preferred_element_type=f32)
        s["shared_hidden"][:, columns] = (jax.nn.silu(gate) * upward).astype(bf16)

    def shared_step(k, carry):
        columns = pl.ds(pl.multiple_of(k * span, span), span)
        shared_out[:, columns] = mixed[:, columns].astype(f32) + jnp.dot(
            s["shared_hidden"][...], s["sd"][:, columns], preferred_element_type=f32
        )
        return carry

    lax.fori_loop(0, width // span, shared_step, 0)

    for dz, r in peers:
        route_copy(dz, r, True).wait_recv()
    for a in range(3):
        landed(trio(1)[a], s["wtr"].at[a])

    def forward(p):
        t = level_at(z, p)
        for c in range(pieces):
            landed(tok.at[t, 0, part(c)], s["zr"].at[t, c])
            spread(tok.at[t, 0, part(c)], t, c)

    def relay(a):
        for k in range(a * WEIGHT_CUTS, (a + 1) * WEIGHT_CUTS):
            target = trio(2)[a]
            size = target.shape[0] // WEIGHT_CUTS
            landed(target.at[pl.ds(k % WEIGHT_CUTS * size, size)], s["wxr"].at[k])
        core_copy(2, a).start()

    expert_lane = lax.broadcasted_iota(jnp.int32, (count, LANES), 1)

    def scale_column(slot, expert):
        table = jnp.concatenate(
            [s["route"][slot], jnp.zeros((LANES - experts, count), f32)], axis=0
        )
        picked = jnp.where(expert_lane == expert, jnp.transpose(table), 0.0)
        return jnp.sum(picked, axis=1, keepdims=True)

    def give(t):
        for c in range(pieces):
            y_copy(t, c).start()

    def y_copy(t, c):
        return remote(
            y_out.at[t, part(c)], y_in.at[t, part(c)], s["rys"].at[t, c], s["ryr"].at[t, c],
            beside,
        )

    hidden = s["hidden"]

    def step(i, carry):
        p = jnp.where(i < 3, i, jnp.where(i == 3, 2, jnp.where(i < 6, 3, 7 - i)))
        e = ((i == 3) | (i > 4)).astype(jnp.int32)
        t = level_at(z, p)

        @pl.when(i == 0)
        def _():
            forward(1)
            forward(2)

        @pl.when(((i == 1) & jnp.logical_not(edge)) | ((i == 2) & edge))
        def _():
            forward(3)

        @pl.when(i == 1)
        def _():
            relay(0)

        @pl.when(i == 2)
        def _():
            relay(1)

        @pl.when(i == 3)
        def _():
            relay(2)
            for a in range(3):
                landed(trio(3)[a], s["wtr"].at[3 + a])

        @pl.when(e == 0)
        def _():
            for c in range(pieces):
                landed(tok.at[t, 1, part(c)], s["yr"].at[t, c])

        expert = jnp.where(e == 0, me, pair)
        scale = jnp.concatenate(
            [scale_column(t * 2, expert), scale_column(t * 2 + 1, expert)], axis=0
        )

        def inner(j, carry):
            block = tok[t].reshape(2 * count, width)
            gate = jnp.dot(block, wg[2 * e + j], preferred_element_type=f32)
            upward = jnp.dot(block, wu[2 * e + j], preferred_element_type=f32)
            columns = pl.ds(pl.multiple_of(j * half, half), half)
            hidden[:, columns] = (jax.nn.silu(gate) * upward * scale).astype(bf16)
            return carry

        lax.fori_loop(0, 2, inner, 0)

        def outer(k, carry):
            columns = pl.ds(pl.multiple_of(k * span, span), span)
            depth = pl.ds(pl.multiple_of(e * 2 * half, 2 * half), 2 * half)
            result = jnp.dot(hidden[...], wd[depth, columns], preferred_element_type=f32)

            @pl.when(e == 0)
            def _():
                acc[t, :, columns] = result

            @pl.when(e == 1)
            def _():
                whole = acc[t, :, columns] + result
                acc[t, :, columns] = whole
                y_out[t, :, columns] = whole[count:].astype(bf16)

            return carry

        lax.fori_loop(0, width // span, outer, 0)

        @pl.when(e == 1)
        def _():
            give(t)

        return carry

    lax.fori_loop(0, 8, step, 0)

    def take(t, c):
        landed(y_in.at[t, part(c)], s["ryr"].at[t, c])

    def arrive(slot, c):
        landed(z_in.at[slot, part(c)], s["rzr"].at[slot, c])

    def hop(p, c):
        t = level_at(z, p)
        up = t > z
        slot = jnp.where(up | (t < z - 1), t, LEVELS)
        return remote(
            z_out.at[t, part(c)],
            z_in.at[slot, part(c)],
            s["rzs"].at[t, c],
            s["rzr"].at[slot, c],
            jnp.where(up, above, below),
        )

    for p in (2, 3, 1):
        t = level_at(z, p)
        up = t > z
        fed = (up & (z > 0)) | (jnp.logical_not(up) & (z < LEVELS - 1))
        for c in range(pieces):
            take(t, c)

            @pl.when(fed)
            def _():
                arrive(t, c)
                z_out[t, part(c)] = (
                    acc[t, part(c)]
                    + y_in[t, part(c)].astype(f32)
                    + z_in[t, part(c)].astype(f32)
                ).astype(bf16)

            @pl.when(jnp.logical_not(fed))
            def _():
                z_out[t, part(c)] = (
                    acc[t, part(c)] + y_in[t, part(c)].astype(f32)
                ).astype(bf16)

            hop(p, c).start()

    for c in range(pieces):
        shared_out[part(c)] += acc[z, part(c)]

        @pl.when(z > 0)
        def _():
            arrive(z, c)
            shared_out[part(c)] += z_in[z, part(c)].astype(f32)

        @pl.when(z < LEVELS - 1)
        def _():
            arrive(LEVELS, c)
            shared_out[part(c)] += z_in[LEVELS, part(c)].astype(f32)

        take(z, c)
        out_ref[part(c)] = (
            shared_out[part(c)] + y_in[z, part(c)].astype(f32)
        ).astype(out_ref.dtype)

    for copy in swaps:
        copy.wait_send()

    @pl.when(x == 0)
    def _():
        query_keep().wait_send()

    @pl.when(x == 1)
    def _():
        query_move(0).wait_send()
        query_move(1).wait_send()
        attended_copy(0, 0).wait_send()

    attended_copy(1, 0).wait_send()
    attended_copy(1, 1).wait_send()
    attended_copy(0, 1).wait_send()
    for k in range(3 * WEIGHT_CUTS):
        weight_piece(k).wait_send()
    for a in range(3):
        core_copy(0, a).wait_send()
        core_copy(2, a).wait_send()
    for dz, r in peers:
        route_copy(dz, r, False).wait_send()

    def drain(t, carry):
        for k in range(2):
            b = chip(t, y, k)

            @pl.when((t <= z) & (z < LEVELS - 1))
            def _():
                kv_along(b, True).wait_send()

            @pl.when((t >= z) & (z > 0))
            def _():
                kv_along(b, False).wait_send()

            kv_across(b).wait_send()
        for c in range(pieces):
            @pl.when((t <= z) & (z < LEVELS - 1))
            def _():
                along(tok.at[t, 0, part(c)], t, c, True).wait_send()

            @pl.when((t >= z) & (z > 0))
            def _():
                along(tok.at[t, 0, part(c)], t, c, False).wait_send()

            across(tok.at[t, 0, part(c)], t, c).wait_send()
            y_copy(t, c).wait_send()
        return carry

    lax.fori_loop(0, LEVELS, drain, 0)
    for p in (1, 2, 3):
        for c in range(pieces):
            hop(p, c).wait_send()


def whole_layer(blocks, vmem_arrays, hbm_arrays, number):
    count, width = vmem_arrays["residual"].shape
    tokens = vmem_arrays["query"].shape[0]
    half = hbm_arrays["gate"].shape[1]
    middle = hbm_arrays["shared_gate"].shape[1]
    heads_width = hbm_arrays["project"].shape[0]
    pieces = 4
    vmem, hbm = pl.BlockSpec(memory_space=pltpu.VMEM), pl.BlockSpec(memory_space=pl.ANY)
    bf16, f32 = jnp.bfloat16, jnp.float32
    dma = pltpu.SemaphoreType.DMA
    scratch = {
        "kv": pltpu.VMEM((blocks, 2, tokens, LANES), bf16),
        "qs": pltpu.VMEM((2, tokens, LANES), bf16),
        "qm": pltpu.VMEM((2, 2, tokens, LANES), bf16),
        "after": pltpu.VMEM((tokens, tokens), bf16),
        "seg": pltpu.VMEM((2, 2 * LEVELS, tokens, LANES), f32),
        "sum": pltpu.VMEM((2, 2 * LEVELS, tokens, LANES), f32),
        "ob": pltpu.VMEM((2, tokens, LANES), bf16),
        "att": pltpu.VMEM((heads_width // LANES, count, LANES), bf16),
        "wo": pltpu.VMEM((heads_width, width), bf16),
        "mixed": pltpu.VMEM((count, width), bf16),
        "normed": pltpu.VMEM((count, width), bf16),
        "tok": pltpu.VMEM((LEVELS, 2, count, width), bf16),
        "acc": pltpu.VMEM((LEVELS, 2 * count, width), f32),
        "wg": pltpu.VMEM((4, width, half), bf16),
        "wu": pltpu.VMEM((4, width, half), bf16),
        "wd": pltpu.VMEM((4 * half, width), bf16),
        "sg": pltpu.VMEM((width, middle), bf16),
        "su": pltpu.VMEM((width, middle), bf16),
        "sd": pltpu.VMEM((middle, width), bf16),
        "shared_out": pltpu.VMEM((count, width), f32),
        "hidden": pltpu.VMEM((2 * count, 2 * half), bf16),
        "shared_hidden": pltpu.VMEM((count, middle), bf16),
        "y_out": pltpu.VMEM((LEVELS, count, width), bf16),
        "y_in": pltpu.VMEM((LEVELS, count, width), bf16),
        "z_out": pltpu.VMEM((LEVELS, count, width), bf16),
        "z_in": pltpu.VMEM((LEVELS + 1, count, width), bf16),
        "route": pltpu.VMEM((2 * LEVELS,) + vmem_arrays["table"].shape, f32),
        "idle": dma((1,)),
        "load_sem": dma((len(hbm_arrays),)),
        "near_sem": dma((3,)),
        "kxs": dma((2,)),
        "kxr": dma((2,)),
        "qss": dma((2,)),
        "qsr": dma((2,)),
        "kzs": dma((2, blocks)),
        "kzr": dma((blocks,)),
        "kys": dma((blocks,)),
        "kyr": dma((blocks,)),
        "oss": dma((2, 2)),
        "osr": dma((4,)),
        "wts": dma((6,)),
        "wtr": dma((6,)),
        "wxs": dma((3 * WEIGHT_CUTS,)),
        "wxr": dma((3 * WEIGHT_CUTS,)),
        "w_send": dma((LEVELS, 2)),
        "w_recv": dma((LEVELS, 2)),
        "zs": dma((2, LEVELS, pieces)),
        "zr": dma((LEVELS, pieces)),
        "ys": dma((LEVELS, pieces)),
        "yr": dma((LEVELS, pieces)),
        "rys": dma((LEVELS, pieces)),
        "ryr": dma((LEVELS, pieces)),
        "rzs": dma((LEVELS, pieces)),
        "rzr": dma((LEVELS + 1, pieces)),
    }
    names = list(vmem_arrays) + list(hbm_arrays) + ["out"] + list(scratch)
    return pl.pallas_call(
        functools.partial(layer_kernel, pieces, names),
        out_shape=jax.ShapeDtypeStruct((count, width), bf16),
        in_specs=[vmem] * len(vmem_arrays) + [hbm] * len(hbm_arrays),
        out_specs=vmem,
        scratch_shapes=list(scratch.values()),
        compiler_params=pltpu.CompilerParams(
            collective_id=number,
            has_side_effects=True,
            vmem_limit_bytes=60 * 1024 * 1024,
        ),
    )(*vmem_arrays.values(), *hbm_arrays.values())


def expert_product(rows, gate_half, up_half, down_half):
    gate = jnp.einsum("seid,edf->seif", rows, gate_half, preferred_element_type=jnp.float32)
    upward = jnp.einsum("seid,edf->seif", rows, up_half, preferred_element_type=jnp.float32)
    hidden = (jax.nn.silu(gate) * upward).astype(jnp.bfloat16)
    return jnp.einsum("seif,efd->seid", hidden, down_half, preferred_element_type=jnp.float32)


def local(
    queries,
    key_rows,
    value_rows,
    residual,
    out_weight,
    norm_gain,
    routes,
    route_weight,
    expert_gate,
    expert_up,
    expert_down,
    shared_gate,
    shared_up,
    shared_down,
):
    query_count = queries.shape[0]
    local_width = queries.shape[1]
    blocks = lax.axis_size("sp")
    experts_all = blocks * expert_gate.shape[0]
    if (
        blocks == 4 * LEVELS
        and expert_gate.shape[0] == 1
        and lax.axis_size("tp") == 2
        and local_width == 2 * LANES
    ):
        picked = routes[:, :, None] == jnp.arange(experts_all, dtype=jnp.int32)
        table = jnp.sum(jnp.where(picked, route_weight[:, :, None], 0.0), axis=1)
        return whole_layer(
            blocks,
            {
                "query": queries,
                "key": key_rows,
                "value": value_rows,
                "residual": residual,
                "gain": norm_gain[None, :],
                "table": table.T,
            },
            {
                "gate": expert_gate[0],
                "up": expert_up[0],
                "down": expert_down[0],
                "project": out_weight,
                "shared_gate": shared_gate,
                "shared_up": shared_up,
                "shared_down": shared_down,
            },
            3,
        )
    kv = jnp.concatenate([key_rows, value_rows], axis=1)
    kv = gather(kv, blocks, 0).reshape(-1, kv.shape[1])
    attended = attention(queries, kv)
    token_rows = residual.shape[0]
    weight_rows = lax.dynamic_slice_in_dim(
        out_weight, lax.axis_index("tp") * local_width, local_width, 0
    )
    projected = lax.psum_scatter(
        jnp.dot(attended, weight_rows, preferred_element_type=jnp.float32),
        "tp",
        scatter_dimension=0,
        tiled=True,
    )
    mixed_wide = (residual.astype(jnp.float32) + projected).astype(jnp.bfloat16).astype(jnp.float32)
    inverse = lax.rsqrt(jnp.mean(mixed_wide * mixed_wide, axis=1, keepdims=True) + norm_eps)
    normed = (mixed_wide * inverse * norm_gain).astype(jnp.bfloat16)
    width = normed.shape[1]
    local_experts = expert_gate.shape[0]
    experts_all = blocks * local_experts
    capacity = max(2, token_rows * TOPK * 5 // (4 * experts_all))
    flat_routes = routes.reshape(-1)
    picks = (flat_routes[:, None] == jnp.arange(experts_all, dtype=jnp.int32)[None, :]).astype(
        jnp.int32
    )
    earlier = jnp.cumsum(picks, axis=0) - picks
    position = flat_routes * capacity + jnp.sum(earlier * picks, axis=1)
    filler = (
        jnp.zeros((experts_all * capacity,), jnp.int32)
        .at[position]
        .set(jnp.arange(flat_routes.shape[0], dtype=jnp.int32) + 1)
    )
    occupied = filler > 0
    source_token = jnp.maximum(filler - 1, 0) // TOPK
    outgoing = jnp.where(
        occupied[:, None], normed[source_token], jnp.zeros((), jnp.bfloat16)
    ).reshape(experts_all, capacity, width)
    both = lax.all_gather(
        exchange(
            outgoing.reshape(blocks, local_experts * capacity, width), blocks, 1
        ).reshape(outgoing.shape),
        "tp",
        axis=0,
        tiled=True,
    )
    shaped = both.reshape(-1, local_experts, both.shape[1], both.shape[2])
    pieces = expert_product(shaped, expert_gate, expert_up, expert_down).reshape(both.shape)
    summed = lax.psum_scatter(pieces.astype(jnp.bfloat16), "tp", scatter_dimension=0, tiled=True)
    results = exchange(
        summed.reshape(blocks, local_experts * capacity, width), blocks, 2
    ).reshape(
        experts_all * capacity, width
    )
    picked = results[position].reshape(token_rows, TOPK, width)
    routed = jnp.sum(picked.astype(jnp.float32) * route_weight[:, :, None], axis=1)
    shared_gate_out = jnp.dot(normed, shared_gate, preferred_element_type=jnp.float32)
    shared_up_out = jnp.dot(normed, shared_up, preferred_element_type=jnp.float32)
    shared_act = (jax.nn.silu(shared_gate_out) * shared_up_out).astype(jnp.bfloat16)
    shared_out = jnp.dot(shared_act, shared_down, preferred_element_type=jnp.float32)
    return (mixed_wide + routed + shared_out).astype(jnp.bfloat16)


def solution(mesh):
    return jax.shard_map(
        local,
        mesh=mesh,
        in_specs=(
            P("sp", "tp"),
            P("sp", "tp"),
            P("sp", "tp"),
            P(("sp", "tp"), None),
            P(),
            P(),
            P(("sp", "tp"), None),
            P(("sp", "tp"), None),
            P("sp", None, "tp"),
            P("sp", None, "tp"),
            P("sp", "tp", None),
            P(),
            P(),
            P(),
        ),
        out_specs=P(("sp", "tp"), None),
        check_vma=False,
    )
```

```python
import functools

import jax
import jax.numpy as jnp
from jax import lax
from jax.experimental import pallas as pl
from jax.experimental.pallas import tpu as pltpu
from jax.sharding import PartitionSpec as P

HEAD_DIM = 64
TOPK = 8


norm_eps = 1e-06


MESH = pl.DeviceIdType.MESH
LANES = 128


def attention_kernel(query_ref, kv_ref, out_ref, acc_ref, later_ref):
    own = lax.axis_index("sp")
    count, width = query_ref.shape
    lane = lax.broadcasted_iota(jnp.int32, (count, LANES), 1)
    row = lax.broadcasted_iota(jnp.int32, (count, count), 0)
    column = lax.broadcasted_iota(jnp.int32, (count, count), 1)
    after = (row > column).astype(jnp.bfloat16)
    acc_ref[...] = jnp.zeros_like(acc_ref)
    later_ref[...] = jnp.zeros_like(later_ref)

    def tile(block, diagonal):
        rows = pl.ds(pl.multiple_of(block * count, count), count)
        for pair in range(width // LANES):
            columns = slice(pair * LANES, (pair + 1) * LANES)
            keys = kv_ref[rows, columns]
            values = kv_ref[rows, width + pair * LANES : width + (pair + 1) * LANES]
            sides = []
            for side in range(LANES // HEAD_DIM):
                head = pair * (LANES // HEAD_DIM) + side
                mine = (lane >= side * HEAD_DIM) & (lane < (side + 1) * HEAD_DIM)
                query = query_ref[:, columns].astype(jnp.float32) * HEAD_DIM ** (-0.5)
                query = jnp.where(mine, query, 0.0).astype(jnp.bfloat16)
                scores = lax.dot_general(
                    query, keys, (((1,), (1,)), ((), ())), preferred_element_type=jnp.float32
                )
                tail = jnp.log(1.0 + jnp.exp(-jnp.abs(scores)))
                cost = jnp.maximum(scores, 0.0) + tail
                if diagonal:
                    cost = jnp.where(column < row, cost, 0.0)
                high = cost.astype(jnp.bfloat16)
                low = (cost - high.astype(jnp.float32)).astype(jnp.bfloat16)
                inside = jnp.dot(high, after, preferred_element_type=jnp.float32)
                inside = inside + jnp.dot(low, after, preferred_element_type=jnp.float32)
                weight = jnp.exp(jnp.minimum(scores, 0.0) - tail - inside)
                if diagonal:
                    weight = jnp.where(column < row, weight, 0.0)
                partial = jnp.dot(
                    weight.astype(jnp.bfloat16), values, preferred_element_type=jnp.float32
                )
                later = later_ref[head]
                sides.append(jnp.exp(-later) * partial)
                total = inside[:, 0:1] + cost[:, 0:1]
                later_ref[head] = later + jnp.broadcast_to(total, later.shape)
            acc_ref[:, columns] += jnp.where(lane < HEAD_DIM, sides[0], sides[1])

    tile(own, True)

    def step(index, carry):
        tile(own - 1 - index, False)
        return carry

    lax.fori_loop(0, own, step, 0)
    out_ref[...] = acc_ref[...].astype(out_ref.dtype)


def attention(queries, kv):
    count, width = queries.shape
    return pl.pallas_call(
        attention_kernel,
        out_shape=jax.ShapeDtypeStruct((count, width), jnp.bfloat16),
        in_specs=[pl.BlockSpec(memory_space=pltpu.VMEM)] * 2,
        out_specs=pl.BlockSpec(memory_space=pltpu.VMEM),
        scratch_shapes=[
            pltpu.VMEM((count, width), jnp.float32),
            pltpu.VMEM((width // HEAD_DIM, count, LANES), jnp.float32),
        ],
        compiler_params=pltpu.CompilerParams(vmem_limit_bytes=56 * 1024 * 1024),
    )(queries, kv)


def gather_kernel(n, depth, in_ref, out_ref, stage, send_sem, recv_sem, local_sem):
    me = lax.axis_index("sp")
    plane = n // depth
    level, place = me // plane, lax.rem(me, plane)

    def above(k):
        return lax.rem(level + k, depth) * plane + place

    def beside(j):
        return level * plane + lax.rem(place + j, plane)

    peers = [above(k) for k in range(1, depth)] + [beside(j) for j in range(1, plane)]
    barrier = pltpu.get_barrier_semaphore()
    for peer in peers:
        pl.semaphore_signal(barrier, inc=1, device_id={"sp": peer}, device_id_type=MESH)
    pl.semaphore_wait(barrier, len(peers))

    def send(source, block, peer, k, j):
        copy = pltpu.make_async_remote_copy(
            src_ref=source,
            dst_ref=out_ref.at[block],
            send_sem=send_sem.at[k, j],
            recv_sem=recv_sem.at[k, j],
            device_id={"sp": peer},
            device_id_type=MESH,
        )
        copy.start()
        return copy

    rising = [send(in_ref, me, above(k), k, 0) for k in range(1, depth)]
    level_copies = [send(in_ref, me, beside(j), 0, j) for j in range(1, plane)]
    inward = pltpu.make_async_copy(in_ref, stage, local_sem)
    inward.start()
    inward.wait()
    outward = pltpu.make_async_copy(stage, out_ref.at[me], local_sem)
    outward.start()
    outward.wait()
    for k in range(1, depth):
        rising[k - 1].wait_recv()
        block = lax.rem(level + depth - k, depth) * plane + place
        for j in range(1, plane):
            level_copies.append(send(out_ref.at[block], block, beside(j), k, j))
    for copy in rising:
        copy.wait_send()
    for copy in level_copies:
        copy.wait()


def gather(array, n, number):
    depth = 4 if n % 4 == 0 else 1
    return pl.pallas_call(
        functools.partial(gather_kernel, n, depth),
        out_shape=jax.ShapeDtypeStruct((n,) + array.shape, array.dtype),
        in_specs=[pl.BlockSpec(memory_space=pltpu.HBM)],
        out_specs=pl.BlockSpec(memory_space=pltpu.HBM),
        scratch_shapes=[
            pltpu.VMEM(array.shape, array.dtype),
            pltpu.SemaphoreType.DMA((depth, n // depth)),
            pltpu.SemaphoreType.DMA((depth, n // depth)),
            pltpu.SemaphoreType.DMA,
        ],
        compiler_params=pltpu.CompilerParams(collective_id=number, has_side_effects=True),
    )(array)


def exchange_kernel(n, in_ref, out_ref, stage, send_sem, recv_sem, local_sem):
    me = lax.axis_index("sp")
    barrier = pltpu.get_barrier_semaphore()
    for k in range(1, n):
        pl.semaphore_signal(
            barrier, inc=1, device_id={"sp": lax.rem(me + k, n)}, device_id_type=MESH
        )
    pl.semaphore_wait(barrier, n - 1)

    def part(peer):
        return in_ref.at[peer]

    copies = []
    for k in range(1, n):
        peer = lax.rem(me + k, n)
        copy = pltpu.make_async_remote_copy(
            src_ref=part(peer),
            dst_ref=out_ref.at[me],
            send_sem=send_sem.at[k],
            recv_sem=recv_sem.at[k],
            device_id={"sp": peer},
            device_id_type=MESH,
        )
        copy.start()
        copies.append(copy)
    inward = pltpu.make_async_copy(part(me), stage, local_sem)
    inward.start()
    inward.wait()
    outward = pltpu.make_async_copy(stage, out_ref.at[me], local_sem)
    outward.start()
    outward.wait()
    for copy in copies:
        copy.wait()


def exchange(array, n, number):
    shape = array.shape[1:]
    return pl.pallas_call(
        functools.partial(exchange_kernel, n),
        out_shape=jax.ShapeDtypeStruct((n,) + shape, array.dtype),
        in_specs=[pl.BlockSpec(memory_space=pltpu.HBM)],
        out_specs=pl.BlockSpec(memory_space=pltpu.HBM),
        scratch_shapes=[
            pltpu.VMEM(shape, array.dtype),
            pltpu.SemaphoreType.DMA((n,)),
            pltpu.SemaphoreType.DMA((n,)),
            pltpu.SemaphoreType.DMA,
        ],
        compiler_params=pltpu.CompilerParams(collective_id=number, has_side_effects=True),
    )(array)


LEVELS = 4
EARLY_PIECES = 2
FIRST_SHIPPED = 4
SHIPPED = 11
SHIP_RATE = 2
WEIGHT_CUTS = 8


def level_at(z, p):
    low = z * 2 < LEVELS
    place = jnp.where(low, z, LEVELS - 1 - z)
    step = jnp.where(p == 0, place, jnp.where(p - 1 < place, p - 1, p))
    return jnp.where(low, step, LEVELS - 1 - step)


def layer_kernel(pieces, names, *refs):
    s = dict(zip(names, refs))
    f32, bf16 = jnp.float32, jnp.bfloat16
    me, core = lax.axis_index("sp"), lax.axis_index("tp")
    x, y, z = lax.rem(me, 2), lax.rem(me // 2, 2), me // 4
    out_ref = s["out"]
    count, width = out_ref.shape
    tokens = s["query"].shape[0]
    blocks = s["kv"].shape[0]
    experts = s["table"].shape[0]
    half = s["wg"].shape[2]
    rows = count // pieces
    span = min(width, 512)

    def chip(level, side, place):
        return level * 4 + side * 2 + place

    def remote(source, target, send, recv, peer, peer_core=None):
        return pltpu.make_async_remote_copy(
            src_ref=source,
            dst_ref=target,
            send_sem=send,
            recv_sem=recv,
            device_id={"sp": peer, "tp": core if peer_core is None else peer_core},
            device_id_type=MESH,
        )

    pair = me + 1 - 2 * x
    beside = chip(z, 1 - y, x)
    above, below = me + 4, me - 4
    mirror = chip(LEVELS - 1 - z, 1 - y, 0)

    def landed(target, recv):
        remote(target, target, s["idle"].at[0], recv, beside).wait_recv()

    wg, wu, wd = s["wg"], s["wu"], s["wd"]

    def trio(j):
        return wg.at[j], wu.at[j], wd.at[pl.ds(j * half, half)]

    loads = list(zip((s["gate"], s["up"], s["down"]), trio(0)))
    loads += [(s["project"], s["wo"])]
    loads += list(zip((s["shared_gate"], s["shared_up"], s["shared_down"]), (s["sg"], s["su"], s["sd"])))
    loads = [
        pltpu.make_async_copy(source, target, s["load_sem"].at[k])
        for k, (source, target) in enumerate(loads)
    ]
    for load in loads:
        load.start()

    def lanes(place):
        return pl.ds(pl.multiple_of(place * LANES, LANES), LANES)

    kv = s["kv"]
    near = [
        pltpu.make_async_copy(s[name].at[:, lanes(x)], kv.at[me, k], s["near_sem"].at[k])
        for k, name in enumerate(("key", "value"))
    ]
    for copy in near:
        copy.start()

    name = lax.broadcasted_iota(jnp.int32, (experts, count), 0)
    table = jnp.zeros((experts, count), f32)
    for k in range(s["chosen"].shape[0]):
        mine = s["chosen"][k : k + 1] == name
        table = table + jnp.where(mine, s["chosen_weight"][k : k + 1], 0.0)
    s["table"][...] = table
    s["route"][z * 2] = table
    row = lax.broadcasted_iota(jnp.int32, (tokens, tokens), 0)
    column = lax.broadcasted_iota(jnp.int32, (tokens, tokens), 1)
    for k in range(2):
        s["after"][k * tokens : (k + 1) * tokens] = (row > column).astype(bf16)
    s["seg"][...] = jnp.zeros_like(s["seg"])
    s["sum"][...] = jnp.zeros_like(s["sum"])

    barrier = pltpu.get_barrier_semaphore()
    peers = [(dz, r) for dz in range(LEVELS) for r in range(2) if (dz, r) != (0, 0)]
    greeted = [
        (chip(lax.rem(z + dz, LEVELS), lax.rem(y + r, 2), x), core) for dz, r in peers
    ]
    greeted += [(me, 1 - core), (pair, core), (pair, 1 - core)]
    greeted += [(mirror + x, 1 - core), (mirror + 1 - x, core), (mirror + 1 - x, 1 - core)]
    for peer, peer_core in greeted:
        pl.semaphore_signal(
            barrier, inc=1, device_id={"sp": peer, "tp": peer_core}, device_id_type=MESH
        )
    pl.semaphore_wait(barrier, len(greeted))

    swaps = [
        remote(
            s[name].at[:, lanes(1 - x)], kv.at[me, k], s["kxs"].at[k], s["kxr"].at[k], pair
        )
        for k, name in enumerate(("key", "value"))
    ]
    for copy in swaps:
        copy.start()

    query, qs = s["query"], s["qs"]
    kept = pltpu.make_async_copy(query.at[:, lanes(0)], qs.at[0], s["near_sem"].at[2])

    def query_keep():
        return remote(
            query.at[:, lanes(1)], qs.at[0], s["qss"].at[1], s["qsr"].at[0], pair
        )

    def query_move(place):
        return remote(
            query.at[:, lanes(place)], qs.at[1], s["qss"].at[place], s["qsr"].at[1],
            mirror + place,
        )

    @pl.when(x == 0)
    def _():
        kept.start()
        query_keep().start()

    @pl.when(x == 1)
    def _():
        query_move(0).start()
        query_move(1).start()

    def weight_piece(k):
        a, r = k // WEIGHT_CUTS, k % WEIGHT_CUTS
        source, target = (s["gate"], s["up"], s["down"])[a], trio(2)[a]
        size = source.shape[0] // WEIGHT_CUTS
        cut = pl.ds(r * size, size)
        return remote(source.at[cut], target.at[cut], s["wxs"].at[k], s["wxr"].at[k], pair)

    for k in range(FIRST_SHIPPED):
        weight_piece(k).start()

    def kv_along(b, up):
        return remote(
            kv.at[b], kv.at[b], s["kzs"].at[0 if up else 1, b], s["kzr"].at[b],
            above if up else below,
        )

    def kv_across(b):
        return remote(kv.at[b], kv.at[b], s["kys"].at[b], s["kyr"].at[b], beside)

    def kv_spread(b):
        t = b // 4

        @pl.when((t <= z) & (z < LEVELS - 1))
        def _():
            kv_along(b, True).start()

        @pl.when((t >= z) & (z > 0))
        def _():
            kv_along(b, False).start()

        kv_across(b).start()

    for copy in near:
        copy.wait()
    kv_spread(me)

    def route_copy(dz, r, incoming):
        origin = lax.rem(z + LEVELS - dz, LEVELS) if incoming else z
        peer = chip(lax.rem(z + dz, LEVELS), lax.rem(y + r, 2), x)
        return remote(
            s["table"], s["route"].at[origin * 2 + r], s["w_send"].at[dz, r],
            s["w_recv"].at[dz, r], peer,
        )

    for dz, r in peers:
        route_copy(dz, r, False).start()

    def core_copy(j, a):
        k = 3 * (j // 2) + a
        return remote(
            trio(j)[a], trio(j + 1)[a], s["wts"].at[k], s["wtr"].at[k], me, 1 - core
        )


    for k in range(2):
        landed(kv.at[pair, k], s["kxr"].at[k])
    kv_spread(pair)

    def kv_forward(p, mine):
        b = chip(level_at(z, p), y, x if mine else 1 - x)
        landed(kv.at[b], s["kzr"].at[b])
        kv_spread(b)

    edge = (z == 0) | (z == LEVELS - 1)
    inner_level = jnp.logical_not(edge)
    kv_forward(1, True)

    @pl.when(inner_level)
    def _():
        kv_forward(2, True)

    for load in loads[:3]:
        load.wait()
    for a in range(3):
        core_copy(0, a).start()
    @pl.when(x == 0)
    def _():
        kept.wait()

    @pl.when(x == 1)
    def _():
        landed(qs.at[0], s["qsr"].at[0])

    landed(qs.at[1], s["qsr"].at[1])
    lane = lax.broadcasted_iota(jnp.int32, (tokens, LANES), 1)
    first = lane < HEAD_DIM
    for f in range(2):
        scaled = qs[f].astype(f32) * HEAD_DIM ** (-0.5)
        s["qm"][f, 0] = jnp.where(first, scaled, 0.0).astype(bf16)
        s["qm"][f, 1] = jnp.where(first, 0.0, scaled).astype(bf16)

    def tile(f, t, b, diagonal):
        parts, totals = [], []
        for h in range(2):
            scores = lax.dot_general(
                s["qm"][f, h], kv[b, 0], (((1,), (1,)), ((), ())), preferred_element_type=f32
            )
            tail = jnp.log(1.0 + jnp.exp(-jnp.abs(scores)))
            cost = jnp.maximum(scores, 0.0) + tail
            if diagonal:
                mask = lax.broadcasted_iota(
                    jnp.int32, (tokens, tokens), 1
                ) < lax.broadcasted_iota(jnp.int32, (tokens, tokens), 0)
                cost = jnp.where(mask, cost, 0.0)
            high = cost.astype(bf16)
            low = (cost - high.astype(f32)).astype(bf16)
            inside = jnp.dot(
                jnp.concatenate([high, low], axis=1), s["after"][...],
                preferred_element_type=f32,
            )
            weight = jnp.exp(jnp.minimum(scores, 0.0) - tail - inside)
            if diagonal:
                weight = jnp.where(mask, weight, 0.0)
            parts.append(jnp.dot(weight.astype(bf16), kv[b, 1], preferred_element_type=f32))
            totals.append(inside[:, 0:1] + cost[:, 0:1])
        total = jnp.where(first, totals[0], totals[1])
        s["seg"][f, t] = s["seg"][f, t] * jnp.exp(-total) + jnp.where(first, parts[0], parts[1])
        s["sum"][f, t] += total

    kept_block = chip(z, y, 0)
    order = ((0, 0), (0, 1), (1, 0), (2, 0), (1, 1), (3, 0), (2, 1), (3, 1))

    def attend(i, carry):
        p = functools.reduce(lambda a, k: jnp.where(i == k, order[k][0], a), range(1, 8), 0)
        far = functools.reduce(lambda a, k: jnp.where(i == k, order[k][1], a), range(1, 8), 0)

        @pl.when(i == 1)
        def _():
            kv_forward(1, False)

        for at, far_level, mine in ((1, 2, True), (2, 2, False), (3, 3, True), (4, 3, False)):
            @pl.when((i == at) & edge)
            def _():
                kv_forward(far_level, mine)

        for at, far_level, mine in ((1, 2, False), (2, 3, True), (3, 3, False)):
            @pl.when((i == at) & inner_level)
            def _():
                kv_forward(far_level, mine)

        t = level_at(z, p)
        side = jnp.where(far == 1, 1 - y, y)
        start = chip(t, side, 0)
        segment = start // 2

        @pl.when(far == 1)
        def _():
            for k in range(2):
                landed(kv.at[start + k], s["kyr"].at[start + k])

        def one_query(f, carry):
            block = jnp.where(f == 0, kept_block, blocks - 1 - kept_block)
            full = jnp.clip(block - start, 0, 2)

            def one_key(b, carry):
                tile(f, segment, start + b, False)
                return carry

            lax.fori_loop(0, full, one_key, 0)

            @pl.when((block >= start) & (block < start + 2))
            def _():
                tile(f, segment, block, True)

            return carry

        lax.fori_loop(0, 2, one_query, 0)

        for k in range(FIRST_SHIPPED, SHIPPED):
            @pl.when(i == (k - FIRST_SHIPPED) // SHIP_RATE)
            def _():
                weight_piece(k).start()

        return carry

    lax.fori_loop(0, 2 * LEVELS, attend, 0)

    for f in range(2):
        later = s["sum"][f, 2 * LEVELS - 1]
        value = s["seg"][f, 2 * LEVELS - 1]
        for t in reversed(range(2 * LEVELS - 1)):
            value = value + jnp.exp(-later) * s["seg"][f, t]
            later = later + s["sum"][f, t]
        s["ob"][f] = value.astype(bf16)

    spot = core * 2 + x

    def attended_copy(f, d):
        other = lax.rem(core + d, 2)
        source = s["ob"].at[f, pl.ds(pl.multiple_of(other * count, count), count)]
        target = kept_block if f == 0 else mirror + 1
        return remote(
            source, s["att"].at[spot], s["oss"].at[f, d], s["osr"].at[spot], target, other
        )

    attended_copy(1, 0).start()
    attended_copy(1, 1).start()
    attended_copy(0, 1).start()

    @pl.when(x == 1)
    def _():
        attended_copy(0, 0).start()

    @pl.when(x == 0)
    def _():
        s["att"][spot] = s["ob"][0, pl.ds(pl.multiple_of(core * count, count), count)]

    loads[3].wait()
    for k in range(4):
        @pl.when((x == 1) | (k != spot))
        def _():
            landed(s["att"].at[k], s["osr"].at[k])

    for k in range(SHIPPED, 3 * WEIGHT_CUTS):
        weight_piece(k).start()

    mixed, normed = s["mixed"], s["normed"]
    attended = jnp.concatenate([s["att"][k] for k in range(4)], axis=1)

    def project_step(k, carry):
        columns = pl.ds(pl.multiple_of(k * span, span), span)
        value = s["residual"][:, columns].astype(f32) + jnp.dot(
            attended, s["wo"][:, columns], preferred_element_type=f32
        )
        value = value.astype(bf16)
        mixed[:, columns] = value
        value = value.astype(f32)
        return carry + jnp.sum(value * value, axis=1, keepdims=True)

    squares = lax.fori_loop(0, width // span, project_step, jnp.zeros((count, 1), f32))
    inverse = lax.rsqrt(squares / width + norm_eps)
    for k in range(width // span):
        columns = slice(k * span, (k + 1) * span)
        normed[:, columns] = (
            mixed[:, columns].astype(f32) * inverse * s["gain"][:, columns]
        ).astype(bf16)

    tok, acc = s["tok"], s["acc"]
    y_out, y_in, z_out, z_in = s["y_out"], s["y_in"], s["z_out"], s["z_in"]

    def part(c):
        return pl.ds(c * rows, rows)

    def along(source, t, c, up):
        return remote(
            source,
            tok.at[t, 0, part(c)],
            s["zs"].at[0 if up else 1, t, c],
            s["zr"].at[t, c],
            above if up else below,
        )

    def across(source, t, c):
        return remote(
            source, tok.at[t, 1, part(c)], s["ys"].at[t, c], s["yr"].at[t, c], beside
        )

    def spread(source, t, c):
        @pl.when((t <= z) & (z < LEVELS - 1))
        def _():
            along(source, t, c, True).start()

        @pl.when((t >= z) & (z > 0))
        def _():
            along(source, t, c, False).start()

        across(source, t, c).start()

    tok[z, 0] = normed[...]
    for c in range(pieces):
        spread(normed.at[part(c)], z, c)

    for load in loads[4:]:
        load.wait()
    shared_out = s["shared_out"]
    shared_half = s["sg"].shape[1] // 2
    for j in range(2):
        columns = slice(j * shared_half, (j + 1) * shared_half)
        gate = jnp.dot(normed[...], s["sg"][:, columns], preferred_element_type=f32)
        upward = jnp.dot(normed[...], s["su"][:, columns], preferred_element_type=f32)
        s["shared_hidden"][:, columns] = (jax.nn.silu(gate) * upward).astype(bf16)

    def shared_step(k, carry):
        columns = pl.ds(pl.multiple_of(k * span, span), span)
        shared_out[:, columns] = mixed[:, columns].astype(f32) + jnp.dot(
            s["shared_hidden"][...], s["sd"][:, columns], preferred_element_type=f32
        )
        return carry

    lax.fori_loop(0, width // span, shared_step, 0)

    for dz, r in peers:
        route_copy(dz, r, True).wait_recv()
    for a in range(3):
        landed(trio(1)[a], s["wtr"].at[a])

    def forward(p):
        t = level_at(z, p)
        for c in range(pieces):
            landed(tok.at[t, 0, part(c)], s["zr"].at[t, c])
            spread(tok.at[t, 0, part(c)], t, c)

    def relay(a):
        for k in range(a * WEIGHT_CUTS, (a + 1) * WEIGHT_CUTS):
            target = trio(2)[a]
            size = target.shape[0] // WEIGHT_CUTS
            landed(target.at[pl.ds(k % WEIGHT_CUTS * size, size)], s["wxr"].at[k])
        core_copy(2, a).start()

    expert_lane = lax.broadcasted_iota(jnp.int32, (count, LANES), 1)

    def scale_column(slot, expert):
        table = jnp.concatenate(
            [s["route"][slot], jnp.zeros((LANES - experts, count), f32)], axis=0
        )
        picked = jnp.where(expert_lane == expert, jnp.transpose(table), 0.0)
        return jnp.sum(picked, axis=1, keepdims=True)

    def give(t):
        for c in range(pieces):
            y_copy(t, c).start()

    def y_copy(t, c):
        return remote(
            y_out.at[t, part(c)], y_in.at[t, part(c)], s["rys"].at[t, c], s["ryr"].at[t, c],
            beside,
        )

    hidden = s["hidden"]

    def take(t, c):
        landed(y_in.at[t, part(c)], s["ryr"].at[t, c])

    def arrive(slot, c):
        landed(z_in.at[slot, part(c)], s["rzr"].at[slot, c])

    def hop(p, c):
        t = level_at(z, p)
        up = t > z
        slot = jnp.where(up | (t < z - 1), t, LEVELS)
        return remote(
            z_out.at[t, part(c)],
            z_in.at[slot, part(c)],
            s["rzs"].at[t, c],
            s["rzr"].at[slot, c],
            jnp.where(up, above, below),
        )

    def combine(p, c):
        t = level_at(z, p)
        up = t > z
        fed = (up & (z > 0)) | (jnp.logical_not(up) & (z < LEVELS - 1))
        take(t, c)

        @pl.when(fed)
        def _():
            arrive(t, c)
            z_out[t, part(c)] = (
                acc[t, part(c)]
                + y_in[t, part(c)].astype(f32)
                + z_in[t, part(c)].astype(f32)
            ).astype(bf16)

        @pl.when(jnp.logical_not(fed))
        def _():
            z_out[t, part(c)] = (
                acc[t, part(c)] + y_in[t, part(c)].astype(f32)
            ).astype(bf16)

        hop(p, c).start()

    def step(i, carry):
        p = jnp.where(i < 3, i, jnp.where(i == 3, 2, jnp.where(i < 6, 3, 7 - i)))
        e = ((i == 3) | (i > 4)).astype(jnp.int32)
        t = level_at(z, p)

        @pl.when(i == 0)
        def _():
            forward(1)
            forward(2)

        @pl.when(((i == 1) & jnp.logical_not(edge)) | ((i == 2) & edge))
        def _():
            forward(3)

        @pl.when(i == 1)
        def _():
            relay(0)

        @pl.when(i == 2)
        def _():
            relay(1)

        @pl.when(i == 3)
        def _():
            relay(2)
            for a in range(3):
                landed(trio(3)[a], s["wtr"].at[3 + a])

        @pl.when(i == 6)
        def _():
            for c in range(EARLY_PIECES // 2):
                combine(2, c)

        @pl.when(i == 7)
        def _():
            for c in range(EARLY_PIECES // 2, EARLY_PIECES):
                combine(2, c)

        @pl.when(e == 0)
        def _():
            for c in range(pieces):
                landed(tok.at[t, 1, part(c)], s["yr"].at[t, c])

        expert = jnp.where(e == 0, me, pair)
        scale = jnp.concatenate(
            [scale_column(t * 2, expert), scale_column(t * 2 + 1, expert)], axis=0
        )

        def inner(j, carry):
            block = tok[t].reshape(2 * count, width)
            gate = jnp.dot(block, wg[2 * e + j], preferred_element_type=f32)
            upward = jnp.dot(block, wu[2 * e + j], preferred_element_type=f32)
            columns = pl.ds(pl.multiple_of(j * half, half), half)
            hidden[:, columns] = (jax.nn.silu(gate) * upward * scale).astype(bf16)
            return carry

        lax.fori_loop(0, 2, inner, 0)

        def outer(k, carry):
            columns = pl.ds(pl.multiple_of(k * span, span), span)
            depth = pl.ds(pl.multiple_of(e * 2 * half, 2 * half), 2 * half)
            result = jnp.dot(hidden[...], wd[depth, columns], preferred_element_type=f32)

            @pl.when(e == 0)
            def _():
                acc[t, :, columns] = result

            @pl.when(e == 1)
            def _():
                whole = acc[t, :, columns] + result
                acc[t, :, columns] = whole
                y_out[t, :, columns] = whole[count:].astype(bf16)

            return carry

        lax.fori_loop(0, width // span, outer, 0)

        @pl.when(e == 1)
        def _():
            give(t)

        return carry

    lax.fori_loop(0, 8, step, 0)

    for c in range(EARLY_PIECES, pieces):
        combine(2, c)
    for p in (3, 1):
        for c in range(pieces):
            combine(p, c)

    def stage_copy(c):
        return pltpu.make_async_copy(
            s["stage"].at[part(c)], out_ref.at[part(c)], s["stage_sem"].at[c]
        )

    for c in range(pieces):
        shared_out[part(c)] += acc[z, part(c)]

        @pl.when(z > 0)
        def _():
            arrive(z, c)
            shared_out[part(c)] += z_in[z, part(c)].astype(f32)

        @pl.when(z < LEVELS - 1)
        def _():
            arrive(LEVELS, c)
            shared_out[part(c)] += z_in[LEVELS, part(c)].astype(f32)

        take(z, c)
        s["stage"][part(c)] = (
            shared_out[part(c)] + y_in[z, part(c)].astype(f32)
        ).astype(bf16)
        stage_copy(c).start()

    for c in range(pieces):
        stage_copy(c).wait()
    for copy in swaps:
        copy.wait_send()

    @pl.when(x == 0)
    def _():
        query_keep().wait_send()

    @pl.when(x == 1)
    def _():
        query_move(0).wait_send()
        query_move(1).wait_send()
        attended_copy(0, 0).wait_send()

    attended_copy(1, 0).wait_send()
    attended_copy(1, 1).wait_send()
    attended_copy(0, 1).wait_send()
    for k in range(3 * WEIGHT_CUTS):
        weight_piece(k).wait_send()
    for a in range(3):
        core_copy(0, a).wait_send()
        core_copy(2, a).wait_send()
    for dz, r in peers:
        route_copy(dz, r, False).wait_send()

    def drain(t, carry):
        for k in range(2):
            b = chip(t, y, k)

            @pl.when((t <= z) & (z < LEVELS - 1))
            def _():
                kv_along(b, True).wait_send()

            @pl.when((t >= z) & (z > 0))
            def _():
                kv_along(b, False).wait_send()

            kv_across(b).wait_send()
        for c in range(pieces):
            @pl.when((t <= z) & (z < LEVELS - 1))
            def _():
                along(tok.at[t, 0, part(c)], t, c, True).wait_send()

            @pl.when((t >= z) & (z > 0))
            def _():
                along(tok.at[t, 0, part(c)], t, c, False).wait_send()

            across(tok.at[t, 0, part(c)], t, c).wait_send()
            y_copy(t, c).wait_send()
        return carry

    lax.fori_loop(0, LEVELS, drain, 0)
    for p in (1, 2, 3):
        for c in range(pieces):
            hop(p, c).wait_send()


def whole_layer(blocks, vmem_arrays, hbm_arrays, number):
    count, width = vmem_arrays["residual"].shape
    tokens = vmem_arrays["query"].shape[0]
    half = hbm_arrays["gate"].shape[1]
    middle = hbm_arrays["shared_gate"].shape[1]
    heads_width = hbm_arrays["project"].shape[0]
    pieces = 4
    vmem, hbm = pl.BlockSpec(memory_space=pltpu.VMEM), pl.BlockSpec(memory_space=pl.ANY)
    bf16, f32 = jnp.bfloat16, jnp.float32
    dma = pltpu.SemaphoreType.DMA
    scratch = {
        "kv": pltpu.VMEM((blocks, 2, tokens, LANES), bf16),
        "qs": pltpu.VMEM((2, tokens, LANES), bf16),
        "qm": pltpu.VMEM((2, 2, tokens, LANES), bf16),
        "after": pltpu.VMEM((2 * tokens, tokens), bf16),
        "table": pltpu.VMEM((blocks, count), f32),
        "seg": pltpu.VMEM((2, 2 * LEVELS, tokens, LANES), f32),
        "sum": pltpu.VMEM((2, 2 * LEVELS, tokens, LANES), f32),
        "ob": pltpu.VMEM((2, tokens, LANES), bf16),
        "att": pltpu.VMEM((heads_width // LANES, count, LANES), bf16),
        "wo": pltpu.VMEM((heads_width, width), bf16),
        "mixed": pltpu.VMEM((count, width), bf16),
        "normed": pltpu.VMEM((count, width), bf16),
        "tok": pltpu.VMEM((LEVELS, 2, count, width), bf16),
        "acc": pltpu.VMEM((LEVELS, 2 * count, width), f32),
        "wg": pltpu.VMEM((4, width, half), bf16),
        "wu": pltpu.VMEM((4, width, half), bf16),
        "wd": pltpu.VMEM((4 * half, width), bf16),
        "sg": pltpu.VMEM((width, middle), bf16),
        "su": pltpu.VMEM((width, middle), bf16),
        "sd": pltpu.VMEM((middle, width), bf16),
        "shared_out": pltpu.VMEM((count, width), f32),
        "hidden": pltpu.VMEM((2 * count, 2 * half), bf16),
        "shared_hidden": pltpu.VMEM((count, middle), bf16),
        "y_out": pltpu.VMEM((LEVELS, count, width), bf16),
        "y_in": pltpu.VMEM((LEVELS, count, width), bf16),
        "z_out": pltpu.VMEM((LEVELS, count, width), bf16),
        "z_in": pltpu.VMEM((LEVELS + 1, count, width), bf16),
        "route": pltpu.VMEM((2 * LEVELS, blocks, count), f32),
        "stage": pltpu.VMEM((count, width), bf16),
        "stage_sem": dma((pieces,)),
        "idle": dma((1,)),
        "load_sem": dma((len(hbm_arrays),)),
        "near_sem": dma((3,)),
        "kxs": dma((2,)),
        "kxr": dma((2,)),
        "qss": dma((2,)),
        "qsr": dma((2,)),
        "kzs": dma((2, blocks)),
        "kzr": dma((blocks,)),
        "kys": dma((blocks,)),
        "kyr": dma((blocks,)),
        "oss": dma((2, 2)),
        "osr": dma((4,)),
        "wts": dma((6,)),
        "wtr": dma((6,)),
        "wxs": dma((3 * WEIGHT_CUTS,)),
        "wxr": dma((3 * WEIGHT_CUTS,)),
        "w_send": dma((LEVELS, 2)),
        "w_recv": dma((LEVELS, 2)),
        "zs": dma((2, LEVELS, pieces)),
        "zr": dma((LEVELS, pieces)),
        "ys": dma((LEVELS, pieces)),
        "yr": dma((LEVELS, pieces)),
        "rys": dma((LEVELS, pieces)),
        "ryr": dma((LEVELS, pieces)),
        "rzs": dma((LEVELS, pieces)),
        "rzr": dma((LEVELS + 1, pieces)),
    }
    names = list(vmem_arrays) + list(hbm_arrays) + ["out"] + list(scratch)
    return pl.pallas_call(
        functools.partial(layer_kernel, pieces, names),
        out_shape=jax.ShapeDtypeStruct((count, width), bf16),
        in_specs=[vmem] * len(vmem_arrays) + [hbm] * len(hbm_arrays),
        out_specs=hbm,
        scratch_shapes=list(scratch.values()),
        compiler_params=pltpu.CompilerParams(
            collective_id=number,
            has_side_effects=True,
            vmem_limit_bytes=60 * 1024 * 1024,
        ),
    )(*vmem_arrays.values(), *hbm_arrays.values())


def expert_product(rows, gate_half, up_half, down_half):
    gate = jnp.einsum("seid,edf->seif", rows, gate_half, preferred_element_type=jnp.float32)
    upward = jnp.einsum("seid,edf->seif", rows, up_half, preferred_element_type=jnp.float32)
    hidden = (jax.nn.silu(gate) * upward).astype(jnp.bfloat16)
    return jnp.einsum("seif,efd->seid", hidden, down_half, preferred_element_type=jnp.float32)


def local(
    queries,
    key_rows,
    value_rows,
    residual,
    out_weight,
    norm_gain,
    routes,
    route_weight,
    expert_gate,
    expert_up,
    expert_down,
    shared_gate,
    shared_up,
    shared_down,
):
    query_count = queries.shape[0]
    local_width = queries.shape[1]
    blocks = lax.axis_size("sp")
    experts_all = blocks * expert_gate.shape[0]
    if (
        blocks == 4 * LEVELS
        and expert_gate.shape[0] == 1
        and lax.axis_size("tp") == 2
        and local_width == 2 * LANES
    ):
        return whole_layer(
            blocks,
            {
                "query": queries,
                "key": key_rows,
                "value": value_rows,
                "residual": residual,
                "gain": norm_gain[None, :],
                "chosen": routes.T,
                "chosen_weight": route_weight.T,
            },
            {
                "gate": expert_gate[0],
                "up": expert_up[0],
                "down": expert_down[0],
                "project": out_weight,
                "shared_gate": shared_gate,
                "shared_up": shared_up,
                "shared_down": shared_down,
            },
            3,
        )
    kv = jnp.concatenate([key_rows, value_rows], axis=1)
    kv = gather(kv, blocks, 0).reshape(-1, kv.shape[1])
    attended = attention(queries, kv)
    token_rows = residual.shape[0]
    weight_rows = lax.dynamic_slice_in_dim(
        out_weight, lax.axis_index("tp") * local_width, local_width, 0
    )
    projected = lax.psum_scatter(
        jnp.dot(attended, weight_rows, preferred_element_type=jnp.float32),
        "tp",
        scatter_dimension=0,
        tiled=True,
    )
    mixed_wide = (residual.astype(jnp.float32) + projected).astype(jnp.bfloat16).astype(jnp.float32)
    inverse = lax.rsqrt(jnp.mean(mixed_wide * mixed_wide, axis=1, keepdims=True) + norm_eps)
    normed = (mixed_wide * inverse * norm_gain).astype(jnp.bfloat16)
    width = normed.shape[1]
    local_experts = expert_gate.shape[0]
    experts_all = blocks * local_experts
    capacity = max(2, token_rows * TOPK * 5 // (4 * experts_all))
    flat_routes = routes.reshape(-1)
    picks = (flat_routes[:, None] == jnp.arange(experts_all, dtype=jnp.int32)[None, :]).astype(
        jnp.int32
    )
    earlier = jnp.cumsum(picks, axis=0) - picks
    position = flat_routes * capacity + jnp.sum(earlier * picks, axis=1)
    filler = (
        jnp.zeros((experts_all * capacity,), jnp.int32)
        .at[position]
        .set(jnp.arange(flat_routes.shape[0], dtype=jnp.int32) + 1)
    )
    occupied = filler > 0
    source_token = jnp.maximum(filler - 1, 0) // TOPK
    outgoing = jnp.where(
        occupied[:, None], normed[source_token], jnp.zeros((), jnp.bfloat16)
    ).reshape(experts_all, capacity, width)
    both = lax.all_gather(
        exchange(
            outgoing.reshape(blocks, local_experts * capacity, width), blocks, 1
        ).reshape(outgoing.shape),
        "tp",
        axis=0,
        tiled=True,
    )
    shaped = both.reshape(-1, local_experts, both.shape[1], both.shape[2])
    pieces = expert_product(shaped, expert_gate, expert_up, expert_down).reshape(both.shape)
    summed = lax.psum_scatter(pieces.astype(jnp.bfloat16), "tp", scatter_dimension=0, tiled=True)
    results = exchange(
        summed.reshape(blocks, local_experts * capacity, width), blocks, 2
    ).reshape(
        experts_all * capacity, width
    )
    picked = results[position].reshape(token_rows, TOPK, width)
    routed = jnp.sum(picked.astype(jnp.float32) * route_weight[:, :, None], axis=1)
    shared_gate_out = jnp.dot(normed, shared_gate, preferred_element_type=jnp.float32)
    shared_up_out = jnp.dot(normed, shared_up, preferred_element_type=jnp.float32)
    shared_act = (jax.nn.silu(shared_gate_out) * shared_up_out).astype(jnp.bfloat16)
    shared_out = jnp.dot(shared_act, shared_down, preferred_element_type=jnp.float32)
    return (mixed_wide + routed + shared_out).astype(jnp.bfloat16)


def solution(mesh):
    return jax.shard_map(
        local,
        mesh=mesh,
        in_specs=(
            P("sp", "tp"),
            P("sp", "tp"),
            P("sp", "tp"),
            P(("sp", "tp"), None),
            P(),
            P(),
            P(("sp", "tp"), None),
            P(("sp", "tp"), None),
            P("sp", None, "tp"),
            P("sp", None, "tp"),
            P("sp", "tp", None),
            P(),
            P(),
            P(),
        ),
        out_specs=P(("sp", "tp"), None),
        check_vma=False,
    )
```
